256 devices in a mesh: grp: 2 (over y), sp: 32 (over z, core), tp: 4 (over x).
Axes of the slice: x: 4, y: 2, z: 16, core: 2. Of those that a mesh axis runs over, the one named last changes fastest.
The devices are a block of a 4x16x16 slice.
Arguments:
- queries: bfloat16 [32768, 1024], P(('grp', 'sp'), 'tp'), parts along dimension 0, may hold values from -6 to 6
- keys: bfloat16 [32768, 1024], P(('grp', 'sp'), 'tp'), parts along dimension 0, may hold values from -6 to 6
- values: bfloat16 [32768, 2048], P(('grp', 'sp'), 'tp'), parts along dimension 0, may hold values from -6 to 6
- in_gate: float32 [8, 32768], P('tp', ('grp', 'sp')), parts along dimension 1, may hold values from -4 to 220
- forget_gate: float32 [8, 32768], P('tp', ('grp', 'sp')), parts along dimension 1, may hold values from 0 to 16
- head_gain: float32 [2048], P('tp'), may hold values from 0.1 to 1.9
- out_weight: bfloat16 [2048, 2048], P('tp'), may hold values from -0.125 to 0.125
- resid: bfloat16 [32768, 2048], P(('grp', 'sp', 'tp')), parts along dimension 0, may hold values from -6 to 6
- norm_gain: float32 [2048], replicated, may hold values from 0.1 to 1.9
- expert_ids: int32 [32768, 2], P(('grp', 'sp', 'tp')), parts along dimension 0, may hold values from 0 to 127, all different within a row; in each aligned block of 128 rows (0 to 127, 128 to 255, ...) at most 8 rows name the same one
- expert_mix: float32 [32768, 2], P(('grp', 'sp', 'tp')), parts along dimension 0, may hold values from 0.25 to 1
- gate_weight: bfloat16 [128, 2048, 512], P(('sp', 'tp')), may hold values from -0.125 to 0.125
- up_weight: bfloat16 [128, 2048, 512], P(('sp', 'tp')), may hold values from -0.125 to 0.125
- down_weight: bfloat16 [128, 512, 2048], P(('sp', 'tp')), may hold values from -0.25 to 0.25
Outputs:
- final: bfloat16 [32768, 2048], P(('grp', 'sp', 'tp')), parts along dimension 0
The draws below stay inside these ranges and needn't reach their ends.
There are 2 independent parts, one for each index of `grp`. The reference program is written for one: setup_inputs(seed, part) draws one part's arguments, and reference() takes and returns one part's arrays. A program takes and returns all parts, laid end to end along the dimension named above; an argument that names none is the same for every part. Nothing has to cross between parts.
Inputs may be any that keep to these rules, and one draw needn't show every extreme that they name: `expert_ids`: each row names 2 different experts. In each aligned block of 128 rows (the rows of one device) no expert is named more than 8 times, a bound that some block reaches.
All inputs are finite; a program needn't handle non-finite values.
Results may differ from the reference program's by a relative error of at most 0.013.
Values may be sent and summed in bfloat16 or wider, within the bound.
No kernel may reach another device: no remote copies, remote signals or barrier semaphores. Data moves between devices by JAX's collectives and lax.ppermute only.
A program may use at most 128 MiB of HBM per device.

```python
import math
import jax
import jax.numpy as jnp
import numpy as np
from jax import lax

D = 2048
HEADS = 8
QK_HEAD = 128
V_HEAD = 256
FF = 512
BLOCK = 128
TOPK = 2
TOK_DEV = 512
TOKENS = 16384
TOK_SHARD = 128
EXPERTS = 128
CAP = 8
N_TP = 4


def draw_in_gate(key, part):
    base_key = jax.random.fold_in(key, 0)
    sample = jnp.clip(jax.random.normal(base_key, (HEADS, TOKENS), jnp.float32), -4.0, 4.0)
    return sample


def draw_forget_gate(key, part):
    order_key, region_key, block_key, noise_key = jax.random.split(key, 4)
    ranks = jax.random.permutation(order_key, HEADS)
    slow = ranks < HEADS // 2
    base = jnp.where(slow, jnp.log(TOKENS / 1.2), jnp.log(40.0)).astype(jnp.float32)
    regions = jax.random.uniform(region_key, (HEADS, TOKENS // TOK_DEV, 1), jnp.float32, -0.8, 0.8)
    regions = jnp.broadcast_to(regions, (HEADS, TOKENS // TOK_DEV, TOK_DEV)).reshape(HEADS, TOKENS)
    blocks = jax.random.uniform(block_key, (HEADS, TOKENS // BLOCK, 1), jnp.float32, -0.3, 0.3)
    blocks = jnp.broadcast_to(blocks, (HEADS, TOKENS // BLOCK, BLOCK)).reshape(HEADS, TOKENS)
    noise = jnp.clip(0.5 * jax.random.normal(noise_key, (HEADS, TOKENS), jnp.float32), -1.5, 1.5)
    return base[:, None] + regions + blocks + noise


def levels(key, shape, pieces, least, largest):
    level, own = 1.0, jax.random.fold_in(key, 6)
    for position, parts in pieces:
        steps = jnp.exp(jax.random.uniform(jax.random.fold_in(own, position), (parts,), jnp.float32, least / len(pieces), largest / len(pieces)))
        level = level * jnp.repeat(steps, shape[position] // parts).reshape([-1 if axis == position else 1 for axis in range(len(shape))])
    return level


def routed_block(stream_key, own, number, rows, number_of, top, reach, slope):
    ranking = jax.random.permutation(stream_key, number_of)
    crowded, common = load_shares(number_of, rows * top, reach, slope, True), load_shares(number_of, rows * top, reach, slope, False)
    places = jnp.arange(number_of)

    def named(tallies, rotation):
        used = int((tallies > 0).sum())
        fixed = max(1, used // 4)
        passed = fixed + (places - fixed + rotation * (used - fixed)) % max(1, number_of - fixed)
        return jnp.zeros((number_of,), jnp.int32).at[ranking[jnp.where(places < fixed, places, passed)]].set(jnp.asarray(tallies, jnp.int32))

    tallies = jnp.where(number % 4 == 0, named(crowded, number // 4), named(common, number - number // 4 - 1))
    mixed = jax.random.permutation(jax.random.fold_in(own, 3), number_of)
    donor, taker = mixed[0:number_of // 2 * 2:2], mixed[1:number_of // 2 * 2:2]
    room = jnp.minimum(tallies[donor] - 1, reach - tallies[taker]) // 2
    room = jnp.where((donor == ranking[0]) | (taker == ranking[0]) | (tallies[taker] == 0), 0, jnp.maximum(room, 0))
    passed = jax.random.randint(jax.random.fold_in(own, 4), (number_of // 2,), 0, 1 << 20) % (room + 1)
    tallies = tallies.at[donor].add(-passed).at[taker].add(passed)
    members = jnp.searchsorted(jnp.cumsum(tallies), jnp.arange(rows * top), side="right").astype(jnp.int32)
    listing = members.reshape(top, rows).T
    listing = listing[jax.random.permutation(jax.random.fold_in(own, 1), rows)]
    rotation = jax.random.randint(jax.random.fold_in(own, 2), (rows, 1), 0, top)
    return jnp.take_along_axis(listing, (jnp.arange(top)[None, :] + rotation) % top, axis=1)


def load_shares(amount, total, bound, slope, full):
    weights = [(1 << 20) // math.isqrt(rank ** slope) + 1 for rank in range(1, amount + 1)]
    largest = bound if full else min(bound, max(-(-total // amount), total * weights[0] // sum(weights)))
    least = 1 if total - largest >= amount - 1 else 0
    counts, surplus = [largest] + [least] * (amount - 1), total - largest - least * (amount - 1)
    while surplus > 0:
        movable = [i for i in range(1, amount) if counts[i] < largest] or [i for i in range(1, amount) if counts[i] < bound]
        pool, left = sum([weights[i] for i in movable]), surplus
        for i in movable:
            addition = min(bound - counts[i], max(1, left * weights[i] // pool), surplus)
            counts[i] = counts[i] + addition
            surplus = surplus - addition
    return np.array(counts)


def normal_values(own_key, shape, deviation, bound, pieces=(), kind=jnp.bfloat16):
    result = jax.random.normal(own_key, shape, jnp.float32) * deviation
    if len(pieces) > 0:
        result = levels(own_key, shape, pieces, -0.22, 0.18) * result
    return jnp.clip(result, min=-bound, max=bound).astype(kind)


def setup_inputs(seed: int = 0, part: int = 0) -> dict:
    splits = jax.random.split(jax.random.key(seed), 15)
    own_keys = jax.random.split(jax.random.fold_in(splits[14], part), 15)
    queries = normal_values(own_keys[0], (TOKENS, HEADS * QK_HEAD), 1.0, 6.0, ((0, 32), (1, 4)))
    keys = normal_values(own_keys[1], (TOKENS, HEADS * QK_HEAD), 1.0, 6.0, ((0, 32), (1, 4)))
    values = normal_values(own_keys[2], (TOKENS, HEADS * V_HEAD), 1.0, 6.0, ((0, 32), (1, 4)))
    in_gate = draw_in_gate(jax.random.fold_in(jax.random.fold_in(splits[14], part), 71), part)
    forget_gate = draw_forget_gate(jax.random.fold_in(jax.random.fold_in(splits[14], part), 71), part)
    head_gain = jnp.clip(1.0 + 0.18 * jax.random.normal(splits[5], (HEADS * V_HEAD,), jnp.float32), 0.1, 1.9)
    out_weight = normal_values(splits[6], (HEADS * V_HEAD, D), (HEADS * V_HEAD) ** -0.5, 0.125, ((0, 4),))
    resid = normal_values(own_keys[7], (TOKENS, D), 1.0, 6.0, ((0, 128),))
    norm_gain = jnp.clip(1.0 + 0.18 * jax.random.normal(splits[8], (D,), jnp.float32), 0.1, 1.9)
    expert_ids_keys = jax.random.split(jax.random.fold_in(own_keys[9], 1), TOKENS // TOK_SHARD)
    expert_ids_turns = jax.random.permutation(jax.random.fold_in(own_keys[9], 3), TOKENS // TOK_SHARD)
    expert_ids = jax.vmap(lambda own, number: routed_block(jax.random.fold_in(own_keys[9], 2), own, number, TOK_SHARD, EXPERTS, TOPK, CAP, 2))(expert_ids_keys, expert_ids_turns).reshape((TOKENS, TOPK))
    expert_mix = jnp.clip(jnp.exp(math.log(1.0) - 1.3862944 * jax.random.uniform(own_keys[10], (TOKENS, TOPK), jnp.float32) ** levels(own_keys[10], (TOKENS, TOPK), ((0, 128),), -0.2, 0.2)), 0.25, 1.0)
    gate_weight = normal_values(splits[11], (EXPERTS, D, FF), D ** -0.5, 0.125, ((0, 128),))
    up_weight = normal_values(splits[12], (EXPERTS, D, FF), D ** -0.5, 0.125, ((0, 128),))
    down_weight = normal_values(splits[13], (EXPERTS, FF, D), FF ** -0.5, 0.25, ((0, 128),))
    return dict(queries=queries, keys=keys, values=values, in_gate=in_gate, forget_gate=forget_gate, head_gain=head_gain, out_weight=out_weight, resid=resid, norm_gain=norm_gain, expert_ids=expert_ids, expert_mix=expert_mix, gate_weight=gate_weight, up_weight=up_weight, down_weight=down_weight)


EPSILON = 1e-06

def head_cell(packed):
    query_heads, keys_h, values_h, in_h, forget_h, gain_h = packed
    count = query_heads.shape[0] // BLOCK
    query_tiles = query_heads.reshape(count, BLOCK, QK_HEAD).astype(jnp.float32)
    key_blocks = keys_h.reshape(count, BLOCK, QK_HEAD).astype(jnp.float32)
    value_tiles = values_h.reshape(count, BLOCK, V_HEAD).astype(jnp.float32)
    in_blocks = in_h.reshape(count, BLOCK)
    log_forget = jax.nn.log_sigmoid(forget_h).reshape(count, BLOCK)
    cumulative = jnp.cumsum(log_forget, axis=1)
    totals = cumulative[:, -1]
    to_end = totals[:, None] - cumulative + in_blocks
    end_max = lax.optimization_barrier(jnp.max(to_end, axis=1))
    key_weighted = (key_blocks * jnp.exp(to_end - end_max[:, None])[:, :, None]).astype(jnp.bfloat16)
    key_forget_weighted = lax.optimization_barrier(key_weighted).astype(jnp.float32)
    state_per_block = jnp.einsum('foj,fop->fjp', value_tiles, key_forget_weighted)

    def advance(carry, input_rows):
        state, stab = carry
        total, bstate, bmax = input_rows
        new_stab = jnp.maximum(total + stab, bmax)
        keep = jnp.exp(total + stab - new_stab)
        added = jnp.exp(bmax - new_stab)
        return ((keep * state + added * bstate, new_stab), (state, stab))
    init = (jnp.zeros((V_HEAD, QK_HEAD), jnp.float32), jnp.zeros((), jnp.float32))
    _, (prev_state, prev_stab) = lax.scan(advance, init, (totals, state_per_block, end_max))
    scale = QK_HEAD ** (-0.5)
    scores = jnp.einsum('ctd,csd->cts', query_tiles, key_blocks) * scale
    causal = jnp.tril(jnp.ones((BLOCK, BLOCK), dtype=bool))
    gaps = cumulative[:, :, None] - cumulative[:, None, :] + in_blocks[:, None, :]
    gaps = jnp.where(causal, gaps, -jnp.inf)
    row_max = lax.optimization_barrier(jnp.max(gaps, axis=2))
    weights = scores * jnp.exp(gaps - row_max[:, :, None])
    rounded = lax.optimization_barrier(weights.astype(jnp.bfloat16)).astype(jnp.float32)
    local_num = jnp.einsum('cts,csv->ctv', rounded, value_tiles)
    inter = cumulative + prev_stab[:, None]
    stab = jnp.maximum(inter, row_max)
    own_scale = jnp.exp(row_max - stab)
    carried = jnp.exp(inter - stab)
    query_scaled = query_tiles * scale
    memory_readout = jnp.einsum('ctk,cvk->ctv', query_scaled, prev_state, precision=lax.Precision.HIGHEST)
    cell = own_scale[..., None] * local_num + carried[..., None] * memory_readout
    cell = cell.reshape(-1, V_HEAD)
    normed = cell * lax.rsqrt(lax.optimization_barrier(jnp.mean(cell * cell, axis=1, keepdims=True)) + EPSILON)
    return normed * gain_h

def reference(queries, keys, values, in_gate, forget_gate, head_gain, out_weight, resid, norm_gain, expert_ids, expert_mix, gate_weight, up_weight, down_weight):
    tokens = queries.shape[0]
    packed = (queries.reshape(tokens, HEADS, QK_HEAD).transpose(1, 0, 2), keys.reshape(tokens, HEADS, QK_HEAD).transpose(1, 0, 2), values.reshape(tokens, HEADS, V_HEAD).transpose(1, 0, 2), in_gate, forget_gate, head_gain.reshape(HEADS, V_HEAD))
    cells = lax.map(head_cell, packed)
    mixed = cells.transpose(1, 0, 2).reshape(tokens, HEADS * V_HEAD).astype(jnp.bfloat16)
    group = HEADS * V_HEAD // N_TP
    proj = jnp.zeros((tokens, D), jnp.float32)
    for group_no in range(N_TP):
        partial_sum = jnp.dot(mixed[:, group_no * group:(group_no + 1) * group], out_weight[group_no * group:(group_no + 1) * group], preferred_element_type=jnp.float32)
        proj = proj + lax.optimization_barrier(partial_sum.astype(jnp.bfloat16)).astype(jnp.float32)
    mid = (resid.astype(jnp.float32) + proj).astype(jnp.bfloat16)
    mid_f = mid.astype(jnp.float32)
    normed = (mid_f * lax.rsqrt(lax.optimization_barrier(jnp.mean(mid_f * mid_f, axis=1, keepdims=True)) + EPSILON) * norm_gain).astype(jnp.bfloat16)
    share = expert_mix / lax.optimization_barrier(jnp.sum(expert_mix, axis=1, keepdims=True))
    flat_ids = expert_ids.reshape(-1)
    flat_share = share.reshape(-1)
    count_all = flat_ids.shape[0]
    order = jnp.argsort(flat_ids, stable=True).astype(jnp.int32)
    loads = jax.ops.segment_sum(jnp.ones_like(flat_ids), flat_ids, num_segments=EXPERTS).astype(jnp.int32)
    starts = (jnp.cumsum(loads) - loads).astype(jnp.int32)
    room = EXPERTS * CAP

    def run_expert(total, expert):
        offsets = jnp.arange(room, dtype=jnp.int32)
        picks = order[jnp.minimum(starts[expert] + offsets, count_all - 1)]
        valid = offsets < loads[expert]
        token_rows = (picks // TOPK).astype(jnp.int32)
        rows = normed[token_rows]
        gate = jnp.dot(rows, gate_weight[expert], preferred_element_type=jnp.float32)
        upper = jnp.dot(rows, up_weight[expert], preferred_element_type=jnp.float32)
        hidden = (jax.nn.silu(gate) * upper).astype(jnp.bfloat16)
        output = jnp.dot(hidden, down_weight[expert], preferred_element_type=jnp.float32).astype(jnp.bfloat16)
        weight = jnp.where(valid, flat_share[picks], 0.0)
        return (total.at[token_rows].add(weight[:, None] * output.astype(jnp.float32)), None)
    total, _ = lax.scan(run_expert, jnp.zeros((tokens, D), jnp.float32), jnp.arange(EXPERTS, dtype=jnp.int32))
    return (mid_f + total).astype(jnp.bfloat16)
```

```python
import functools

import jax
import jax.numpy as jnp
from jax import lax
from jax.experimental import pallas as pl
from jax.experimental.pallas import tpu as pltpu
from jax.sharding import PartitionSpec as P

QK_HEAD = 128
V_HEAD = 256
BLOCK = 128
TOPK = 2
CAP_FACTOR = 4


EPSILON = 1e-06
VERY_LOW = -1e30


def copy_for_each(x, axis):
    count = lax.axis_size(axis)
    return lax.all_to_all(jnp.broadcast_to(x[None], (count, *x.shape)), axis, 0, 0, tiled=True)


def joined_along(parts, dim):
    lengths = list(parts.shape[1:])
    lengths[dim] *= parts.shape[0]
    return jnp.moveaxis(parts, 0, dim).reshape(lengths)


def gather_directly(x, axis, dim):
    parts = copy_for_each(x, axis)
    return joined_along(parts, dim)


def sent_together(arrays, axis, dim, along):
    columns = [a.reshape(*a.shape[:along], -1) for a in arrays]
    both = jnp.concatenate(columns, axis=along)
    whole, at, done = (lax.all_gather(both, axis, axis=dim, tiled=True), 0, [])
    for a, column in zip(arrays, columns):
        section = whole[..., at : at + column.shape[along]]
        done.append(section.reshape(*section.shape[:along], *a.shape[along:]))
        at += column.shape[along]
    return tuple(done)


def in_blocks_2(x, dim, count):
    lengths = x.shape
    parts = x.reshape(*lengths[:dim], count, lengths[dim] // count, *lengths[dim + 1 :])
    return jnp.moveaxis(parts, dim, 0)


def summed_on_arrival(x, axis, dim):
    parts = in_blocks_2(x, dim, lax.axis_size(axis))
    arrived = lax.all_to_all(parts, axis, split_axis=0, concat_axis=0, tiled=True)
    return arrived.astype(jnp.float32).sum(axis=0)


def join_states(before_part, after_part):
    before_total, before_state, before_stab = before_part
    after_total, after_state, after_stab = after_part
    stab = jnp.maximum(before_stab + after_total, after_stab)
    keep = jnp.exp(before_stab + after_total - stab)
    added = jnp.exp(after_stab - stab)
    return (
        before_total + after_total,
        before_state * keep[:, None, None] + after_state * added[:, None, None],
        stab,
    )


def expert_ffn(arrived, gate_weight, up_weight, down_weight):
    width = arrived.shape[-1]
    flat = arrived.reshape(-1, width)
    gate = jnp.dot(flat, gate_weight[0], preferred_element_type=jnp.float32)
    upper = jnp.dot(flat, up_weight[0], preferred_element_type=jnp.float32)
    hidden = (jax.nn.silu(gate) * upper).astype(jnp.bfloat16)
    output = jnp.dot(hidden, down_weight[0], preferred_element_type=jnp.float32).astype(
        jnp.bfloat16
    )
    return output.reshape(arrived.shape)


PLANE_ROWS = 32
GROUP = 4
SLOTS = 8
ORIGINS = (1, 15, 2, 14, 3, 13, 4, 12, 5, 11, 6, 10, 7, 9, 8, 0)
VMEM = pltpu.VMEM


def core_pairs():
    return [(i, i ^ 1) for i in range(lax.axis_size("sp"))]


def ring_shift(step):
    size = lax.axis_size("sp")
    return [(i, (i + (2 * step if i % 2 == 0 else -2 * step)) % size) for i in range(size)]


def lane_shift(step):
    size = lax.axis_size("tp")
    return [(i, (i + step) % size) for i in range(size)]


def earlier(count):
    return jnp.triu(jnp.ones((count, count), jnp.bfloat16), 1)


def ranks(marks):
    rows = marks.reshape(-1, marks.shape[-1]).astype(jnp.bfloat16)
    got = jnp.dot(rows, earlier(marks.shape[-1]), preferred_element_type=jnp.float32)
    return got.reshape(marks.shape)


def route_tables(expert_ids, share):
    tokens = expert_ids.shape[0]
    planes = lax.axis_size("sp") // 2
    lanes = lax.axis_size("tp")
    in_plane = 2 * lanes
    mine, lane = lax.axis_index("sp"), lax.axis_index("tp")
    level, core = mine // 2, mine % 2
    sign = 1 - 2 * core
    meta = jnp.concatenate([expert_ids.T.astype(jnp.float32), share.T], axis=0)
    gathered = copy_for_each(meta, "sp")
    ids_all = gathered[:, :TOPK].astype(jnp.int32)
    share_all = gathered[:, TOPK:]
    needs = jnp.arange(planes, dtype=jnp.int32)[None, :, None]
    named = (ids_all[:, 0:1] // in_plane == needs) | (ids_all[:, 1:2] // in_plane == needs)
    most = jnp.max(jnp.sum(named.astype(jnp.float32), axis=2))
    alone = jnp.broadcast_to((most <= PLANE_ROWS).astype(jnp.float32), (8, 128))
    fits = alone
    for step in range(1, lanes):
        fits = fits * lax.ppermute(alone, "tp", lane_shift(step))
    order = jnp.array(ORIGINS, jnp.int32)
    count = len(ORIGINS)
    sources = 2 * ((level - sign * order) % planes) + core
    ids = ids_all[sources]
    shares = share_all[sources]
    local = ids - in_plane * level
    inside = (local >= 0) & (local < in_plane)
    relx = (local % lanes - lane) % lanes
    relc = (local // lanes) ^ core
    code = jnp.where(inside, relx * 2 + relc, -1)
    which = jnp.arange(in_plane, dtype=jnp.int32)[None, :, None]
    hit0, hit1 = code[:, 0:1] == which, code[:, 1:2] == which
    marks = hit0 | hit1
    weight = jnp.where(hit0, shares[:, 0:1], 0.0) + jnp.where(hit1, shares[:, 1:2], 0.0)
    slot = ranks(marks)
    slot_no = jnp.arange(SLOTS, dtype=jnp.float32)[None, None, :, None]
    placed = (marks[:, :, None] & (slot[:, :, None] == slot_no)).astype(jnp.bfloat16)
    slot_share = jnp.sum(placed.astype(jnp.float32) * weight[:, :, None], axis=3)
    wanted = jnp.any(inside, axis=1)
    row = ranks(wanted)
    row_no = jnp.arange(PLANE_ROWS, dtype=jnp.float32)[None, :, None]
    rows = (wanted[:, None] & (row[:, None] == row_no)).astype(jnp.bfloat16)
    pick = jnp.einsum("ojst,ort->ojsr", placed, rows, preferred_element_type=jnp.float32)
    groups = count // GROUP
    pick = pick.reshape(groups, GROUP, in_plane, SLOTS, PLANE_ROWS)
    eye = jnp.eye(GROUP, dtype=jnp.float32)
    select = jnp.einsum("gojsr,op->gjospr", pick, eye)
    select = select.reshape(groups, in_plane * GROUP * SLOTS, GROUP * PLANE_ROWS)
    slot_share = slot_share.reshape(groups, GROUP, in_plane, SLOTS).transpose(0, 2, 1, 3)
    back = select * slot_share.reshape(groups, -1)[:, :, None]
    back = back.transpose(0, 2, 1)
    high = back.astype(jnp.bfloat16)
    low = (back - high.astype(jnp.float32)).astype(jnp.bfloat16)
    targets = (level + sign * order) % planes
    leaving = jnp.any(expert_ids.T[None] // in_plane == targets[:, None, None], axis=1)
    leave_row = ranks(leaving)
    pack = (leaving[:, None] & (leave_row[:, None] == row_no)).astype(jnp.bfloat16)
    pack = pack.reshape(count * PLANE_ROWS, tokens)
    return fits[0, 0] > 0.5, pack, pack.T, select.astype(jnp.bfloat16), high, low


def matmul(a, b):
    return jnp.dot(a, b, preferred_element_type=jnp.float32)


def pack_kernel(pack_ref, rows_ref, *outs):
    rows = rows_ref[...]
    for number, out in enumerate(outs):
        size = out.shape[0]
        out[...] = matmul(pack_ref[number * size : (number + 1) * size], rows).astype(out.dtype)


def select_kernel(select_ref, *refs):
    ins, outs = refs[:GROUP], refs[GROUP:]
    rows = jnp.concatenate([r[...] for r in ins], axis=0)
    for number, out in enumerate(outs):
        size = out.shape[0]
        out[...] = matmul(select_ref[number * size : (number + 1) * size], rows).astype(out.dtype)


def back_kernel(high_ref, low_ref, *refs):
    lanes = len(refs) - GROUP
    ins, outs = refs[:lanes], refs[lanes:]
    rows = jnp.concatenate([r[...] for r in ins], axis=0)
    for number, out in enumerate(outs):
        size = out.shape[0]
        part = slice(number * size, (number + 1) * size)
        out[...] = (matmul(high_ref[part], rows) + matmul(low_ref[part], rows)).astype(out.dtype)


def final_kernel(pack_ref, mid_ref, *refs):
    ins, out = refs[:-1], refs[-1]
    rows = jnp.concatenate([r[...] for r in ins], axis=0)
    out[...] = (mid_ref[...] + matmul(pack_ref[...], rows)).astype(out.dtype)


def ffn_kernel(lanes, *refs):
    ins, weights = refs[:lanes], refs[lanes : lanes + 6]
    outs, held, sems = refs[lanes + 6 : 2 * lanes + 6], refs[2 * lanes + 6 : 2 * lanes + 12], refs[-1]
    copies = [pltpu.make_async_copy(w, h, sems.at[n]) for n, (w, h) in enumerate(zip(weights, held))]
    for copy in copies:
        copy.start()
    half = ins[0].shape[0] // 2
    for which in range(2):
        part = slice(which * half, (which + 1) * half)
        rows = jnp.concatenate([r[part] for r in ins], axis=0)
        copies[3 * which].wait()
        gate = matmul(rows, held[3 * which][...])
        copies[3 * which + 1].wait()
        upper = matmul(rows, held[3 * which + 1][...])
        hidden = (gate * jax.nn.sigmoid(gate) * upper).astype(jnp.bfloat16)
        copies[3 * which + 2].wait()
        result = matmul(hidden, held[3 * which + 2][...]).astype(jnp.bfloat16)
        for number, out in enumerate(outs):
            out[part] = result[number * half : (number + 1) * half]


def in_vmem(kernel, outs, name, flops, count, scratch=(), specs=None):
    return pl.pallas_call(
        kernel,
        out_shape=outs,
        in_specs=specs or [pl.BlockSpec(memory_space=VMEM)] * count,
        out_specs=[pl.BlockSpec(memory_space=VMEM)] * len(outs),
        scratch_shapes=list(scratch),
        name=name,
        cost_estimate=pl.CostEstimate(flops=flops, bytes_accessed=1 << 21, transcendentals=0),
        compiler_params=pltpu.CompilerParams(vmem_limit_bytes=40 << 20),
    )


def planes_path(normed, mid_f, routing, own, swapped):
    _, pack, unpack, select, high, low = routing
    width = normed.shape[1]
    lanes = lax.axis_size("tp")
    groups = len(ORIGINS) // GROUP
    bf = jnp.bfloat16
    block = jax.ShapeDtypeStruct((PLANE_ROWS, width), bf)
    lane_rows = jax.ShapeDtypeStruct((2 * GROUP * SLOTS, width), bf)
    sent = in_vmem(pack_kernel, [block] * len(ORIGINS), "pack", 1 << 29, 2)(pack, normed)
    arrived = [
        piece if step == 0 else lax.ppermute(piece, "sp", ring_shift(step))
        for step, piece in zip(ORIGINS, sent)
    ]
    weights = [*own, *swapped]
    returned = []
    for group in range(groups):
        chosen = in_vmem(select_kernel, [lane_rows] * lanes, "select", 1 << 28, 1 + GROUP)(
            select[group], *arrived[group * GROUP : (group + 1) * GROUP]
        )
        there = [
            a if step == 0 else lax.ppermute(a, "tp", lane_shift(step)) for step, a in enumerate(chosen)
        ]
        vm, hbm = pl.BlockSpec(memory_space=VMEM), pl.BlockSpec(memory_space=pl.ANY)
        served = in_vmem(
            functools.partial(ffn_kernel, lanes),
            [lane_rows] * lanes,
            "experts",
            1 << 31,
            0,
            scratch=[pltpu.VMEM(w.shape, bf) for w in weights] + [pltpu.SemaphoreType.DMA((6,))],
            specs=[vm] * lanes + [hbm] * 6,
        )(*there, *weights)
        home = [
            a if step == 0 else lax.ppermute(a, "tp", lane_shift(-step)) for step, a in enumerate(served)
        ]
        results = in_vmem(back_kernel, [block] * GROUP, "back", 1 << 29, 2 + lanes)(
            high[group], low[group], *home
        )
        for step, piece in zip(ORIGINS[group * GROUP : (group + 1) * GROUP], results):
            returned.append(piece if step == 0 else lax.ppermute(piece, "sp", ring_shift(-step)))
    out = jax.ShapeDtypeStruct(normed.shape, bf)
    return in_vmem(final_kernel, [out], "final", 1 << 29, 2 + len(returned))(unpack, mid_f, *returned)[0]


def slots_path(normed, mid_f, expert_ids, share, gate_weight, up_weight, down_weight):
    shard = normed.shape[0]
    width = normed.shape[1]
    expert_group = lax.axis_size("sp") * lax.axis_size("tp")
    assigns = expert_ids.reshape(-1)
    assign_count = assigns.shape[0]
    slots_each = CAP_FACTOR * assign_count // expert_group
    one_hot = (assigns[:, None] == jnp.arange(expert_group, dtype=jnp.int32)[None, :]).astype(
        jnp.bfloat16
    )
    earlier_mask = jnp.tril(jnp.ones((assign_count, assign_count), jnp.bfloat16), -1)
    counts_before = jnp.dot(earlier_mask, one_hot, preferred_element_type=jnp.float32)
    slot = jnp.sum(counts_before * one_hot.astype(jnp.float32), axis=1).astype(jnp.int32)
    target = assigns * slots_each + slot
    filler = (
        jnp.full((expert_group * slots_each,), -1, jnp.int32)
        .at[target]
        .set(jnp.arange(assign_count, dtype=jnp.int32))
    )
    rows_from = jnp.maximum(filler, 0) // TOPK
    outgoing = jnp.where((filler >= 0)[:, None], normed[rows_from], jnp.zeros((), jnp.bfloat16))
    outgoing = outgoing.reshape(expert_group, slots_each, width)
    served = expert_ffn(
        lax.all_to_all(outgoing, ("sp", "tp"), split_axis=0, concat_axis=0, tiled=True),
        gate_weight,
        up_weight,
        down_weight,
    )
    returned = lax.all_to_all(served, ("sp", "tp"), split_axis=0, concat_axis=0, tiled=True)
    picked = returned.reshape(expert_group * slots_each, width)[target]
    picked = picked.reshape(shard, TOPK, width).astype(jnp.float32)
    total = jnp.sum(share[:, :, None] * picked, axis=1)
    return (mid_f + total).astype(jnp.bfloat16)


def per_device(
    queries,
    keys,
    values,
    in_gate,
    forget_gate,
    head_gain,
    out_weight,
    resid,
    norm_gain,
    expert_ids,
    expert_mix,
    gate_weight,
    up_weight,
    down_weight,
):
    tokens = queries.shape[0]
    heads = in_gate.shape[0]
    count = tokens // BLOCK
    scale = QK_HEAD ** (-0.5)
    query_tiles = queries.reshape(count, BLOCK, heads, QK_HEAD)
    key_blocks = keys.reshape(count, BLOCK, heads, QK_HEAD)
    value_tiles = values.reshape(count, BLOCK, heads, V_HEAD)
    in_blocks = in_gate.reshape(heads, count, BLOCK)
    cumulative = jnp.cumsum(jax.nn.log_sigmoid(forget_gate).reshape(heads, count, BLOCK), axis=2)
    totals = cumulative[:, :, -1]
    to_end = totals[:, :, None] - cumulative + in_blocks
    end_max = jnp.max(to_end, axis=2)
    end_weight = jnp.exp(to_end - end_max[:, :, None]).transpose(1, 2, 0)
    key_weighted = (key_blocks * end_weight[..., None]).astype(jnp.bfloat16)
    state_per_block = jnp.einsum(
        "clhv,clhk->hcvk", value_tiles, key_weighted, preferred_element_type=jnp.float32
    )
    summary = (totals[:, 0], state_per_block[:, 0], end_max[:, 0])
    for block_no in range(1, count):
        summary = join_states(
            summary, (totals[:, block_no], state_per_block[:, block_no], end_max[:, block_no])
        )
    totals_all = gather_directly(summary[0][None], "sp", 0)
    offsets_cum = jnp.concatenate(
        [jnp.zeros((1, heads), jnp.float32), jnp.cumsum(totals_all, axis=0)], axis=0
    )
    mine = lax.axis_index("sp")
    mine_cum = lax.dynamic_index_in_dim(offsets_cum, mine, 0, keepdims=False)
    state_acc = jnp.zeros_like(summary[1])
    piece_state, piece_stab = sent_together((summary[1][None], summary[2][None]), "sp", 0, 2)
    width = piece_stab.shape[0]
    sources = jnp.arange(width, dtype=jnp.int32)
    after_cum = lax.dynamic_slice_in_dim(offsets_cum, 1, width, 0)
    log_weight = piece_stab + mine_cum[None, :] - after_cum
    log_weight = jnp.where((sources < mine)[:, None], log_weight, VERY_LOW)
    stab = jnp.maximum(mine_cum, jnp.max(log_weight, axis=0))
    absorb_keep = jnp.exp(mine_cum - stab)
    source_weight = jnp.exp(log_weight - stab[None, :])
    new_state = state_acc * absorb_keep[:, None, None] + jnp.einsum(
        "ph,phvk->hvk", source_weight, piece_state, precision=lax.Precision.HIGHEST
    )
    enter_stab = stab
    state, stab = (new_state, enter_stab)
    state_list, stab_list = ([], [])
    for block_no in range(count):
        state_list.append(state)
        stab_list.append(stab)
        new_stab = jnp.maximum(totals[:, block_no] + stab, end_max[:, block_no])
        keep = jnp.exp(totals[:, block_no] + stab - new_stab)
        added = jnp.exp(end_max[:, block_no] - new_stab)
        state = state * keep[:, None, None] + state_per_block[:, block_no] * added[:, None, None]
        stab = new_stab
    prev_state = jnp.stack(state_list, axis=1)
    prev_stab = jnp.stack(stab_list, axis=1)
    scores = (
        jnp.einsum("cthd,cshd->hcts", query_tiles, key_blocks, preferred_element_type=jnp.float32)
        * scale
    )
    causal = jnp.tril(jnp.ones((BLOCK, BLOCK), dtype=bool))
    gaps = cumulative[..., :, None] - cumulative[..., None, :] + in_blocks[..., None, :]
    gaps = jnp.where(causal, gaps, -jnp.inf)
    row_max = jnp.max(gaps, axis=3)
    weights = scores * jnp.exp(gaps - row_max[..., None])
    rounded = weights.astype(jnp.bfloat16)
    local_num = jnp.einsum(
        "hcts,cshv->hctv", rounded, value_tiles, preferred_element_type=jnp.float32
    )
    inter = cumulative + prev_stab[..., None]
    stab_t = jnp.maximum(inter, row_max)
    own_scale = jnp.exp(row_max - stab_t)
    carried = jnp.exp(inter - stab_t)
    query_scaled = query_tiles.astype(jnp.float32) * scale
    memory_readout = jnp.einsum(
        "cthk,hcvk->hctv", query_scaled, prev_state, precision=lax.Precision.HIGHEST
    )
    cell = own_scale[..., None] * local_num + carried[..., None] * memory_readout
    cell = cell * lax.rsqrt(jnp.mean(cell * cell, axis=3, keepdims=True) + EPSILON)
    cell = cell * head_gain.reshape(heads, 1, 1, V_HEAD)
    mixed = cell.transpose(1, 2, 0, 3).reshape(tokens, heads * V_HEAD).astype(jnp.bfloat16)
    shard = tokens // lax.axis_size("tp")
    proj = summed_on_arrival(
        jnp.dot(mixed, out_weight, preferred_element_type=jnp.float32).astype(jnp.bfloat16), "tp", 0
    )
    mid_f = (resid.astype(jnp.float32) + proj).astype(jnp.bfloat16).astype(jnp.float32)
    normed = (
        mid_f * lax.rsqrt(jnp.mean(mid_f * mid_f, axis=1, keepdims=True) + EPSILON) * norm_gain
    ).astype(jnp.bfloat16)
    share = expert_mix / jnp.sum(expert_mix, axis=1, keepdims=True)
    routing = route_tables(expert_ids, share)
    swapped = tuple(lax.ppermute(w[0], "sp", core_pairs()) for w in (gate_weight, up_weight, down_weight))
    own = (gate_weight[0], up_weight[0], down_weight[0])
    return lax.cond(
        routing[0],
        lambda: planes_path(normed, mid_f, routing, own, swapped),
        lambda: slots_path(normed, mid_f, expert_ids, share, gate_weight, up_weight, down_weight),
    )


def solution(mesh):
    in_specs = (
        P(("grp", "sp"), "tp"),
        P(("grp", "sp"), "tp"),
        P(("grp", "sp"), "tp"),
        P("tp", ("grp", "sp")),
        P("tp", ("grp", "sp")),
        P("tp"),
        P("tp", None),
        P(("grp", "sp", "tp"), None),
        P(),
        P(("grp", "sp", "tp"), None),
        P(("grp", "sp", "tp"), None),
        P(("sp", "tp"), None, None),
        P(("sp", "tp"), None, None),
        P(("sp", "tp"), None, None),
    )
    out_specs = P(("grp", "sp", "tp"), None)
    return jax.shard_map(
        per_device, mesh=mesh, in_specs=in_specs, out_specs=out_specs, check_vma=False
    )
```

```python
import functools

import jax
import jax.numpy as jnp
from jax import lax
from jax.experimental import pallas as pl
from jax.experimental.pallas import tpu as pltpu
from jax.sharding import PartitionSpec as P


QK_HEAD = 128
V_HEAD = 256
BLOCK = 128
TOPK = 2
CAP_FACTOR = 4
EPSILON = 1e-06
VERY_LOW = -1e30

PLANE_ROWS = 32
GROUP = 4
SLOTS = 8
ORIGINS = (7, 9, 8, 0, 5, 11, 6, 10, 3, 13, 4, 12, 1, 15, 2, 14)
PLAN = (
    "o2", "o14", "o8", "o9", "o7", "o1", "o15", "o5", "o11", "o6", "o13", "o10", "o12", "S0", "x0", "S3", "o3",
    "o4", "x3", "E0", "h0", "E3", "h3", "B0", "r8", "S1", "x1", "r9", "S2", "r7", "E1", "h1", "x2", "B3", "r15",
    "r2", "B1", "r10", "r5", "E2", "r14", "r6", "h2", "r11", "B2", "r3", "r13", "r4", "r1", "r12",
)

F32, BF16 = jnp.float32, jnp.bfloat16
VMEM = pltpu.VMEM


SUMS = ((0, 1), (2, 3))


def core_pairs():
    return [(i, i ^ 1) for i in range(lax.axis_size("sp"))]


def ring_shift(step):
    size = lax.axis_size("sp")
    return [(i, (i + (2 * step if i % 2 == 0 else -2 * step)) % size) for i in range(size)]


def lane_shift(step):
    size = lax.axis_size("tp")
    return [(i, (i + step) % size) for i in range(size)]


def over_chips(x):
    size = lax.axis_size("sp")
    groups = [list(range(core, size, 2)) for core in range(2)]
    return lax.all_to_all(x, "sp", 0, 0, axis_index_groups=groups, tiled=True)


def call(kernel, outs, operands, flops, after=None, scratch=(), hbm=(), limit=12 << 20):
    specs = [pl.BlockSpec(memory_space=pl.ANY if n in hbm else VMEM) for n in range(len(operands))]
    operands = list(operands)
    if after is not None:
        operands.append(after)
        specs.append(pl.BlockSpec(memory_space=pl.ANY))
    count = len(operands)

    def body(*refs):
        mine = lax.axis_index("sp")
        place = (lax.div(mine, 2), lax.rem(mine, 2), lax.axis_index("tp"))
        kernel(place, *(refs[: count - 1] if after is not None else refs[:count]), *refs[count:])

    return pl.pallas_call(
        body,
        out_shape=outs,
        in_specs=specs,
        out_specs=[pl.BlockSpec(memory_space=VMEM)] * len(outs),
        scratch_shapes=list(scratch),
        cost_estimate=pl.CostEstimate(flops=flops, bytes_accessed=1 << 21, transcendentals=0),
        compiler_params=pltpu.CompilerParams(vmem_limit_bytes=limit),
    )(*operands)


def struct(shape, kind):
    return jax.ShapeDtypeStruct(shape, kind)


def matmul(a, b):
    return jnp.dot(a, b, preferred_element_type=F32)


def parts_of(x):
    high = x.astype(BF16).astype(F32)
    rest = x - high
    middle = rest.astype(BF16).astype(F32)
    return high, middle, (rest - middle).astype(BF16).astype(F32)


def in_two(x):
    high = x.astype(BF16).astype(F32)
    return high, x - high


def iota(shape, dim):
    return lax.broadcasted_iota(jnp.int32, shape, dim)


def fetch(pairs, sems):
    copies = [pltpu.make_async_copy(source, target, sems.at[n]) for n, (source, target) in enumerate(pairs)]
    for copy in copies:
        copy.start()
    return copies


def decays(gate, forget):
    heads, tokens = gate.shape
    count = tokens // BLOCK
    pieces = [(h, b) for h in range(heads) for b in range(count)]

    def cut(whole):
        return jnp.concatenate([whole[h : h + 1, b * BLOCK : (b + 1) * BLOCK] for h, b in pieces], axis=0)

    forget, gate = cut(forget), cut(gate)
    small = jnp.exp(-jnp.abs(forget))
    one_up = 1.0 + small
    exact = one_up == 1.0
    log_up = jnp.where(exact, small, jnp.log(one_up) * small / jnp.where(exact, 1.0, one_up - 1.0))
    log_forget = jnp.minimum(forget, 0.0) - log_up
    upto = (iota((BLOCK, BLOCK), 0) <= iota((BLOCK, BLOCK), 1)).astype(BF16)
    cumulative = sum(matmul(p.astype(BF16), upto) for p in parts_of(log_forget))
    total = cumulative[:, BLOCK - 1 : BLOCK]
    to_end = total - cumulative + gate
    top = jnp.max(to_end, axis=1, keepdims=True)
    return cumulative, gate, total, jnp.exp(to_end - top), top


def fetch(pairs, sems):
    copies = [pltpu.make_async_copy(source, target, sems.at[n]) for n, (source, target) in enumerate(pairs)]
    for copy in copies:
        copy.start()
    return copies


def state_of(k_ref, v_ref, weight, h, b, r):
    keys = k_ref[b * BLOCK : (b + 1) * BLOCK, h * QK_HEAD : (h + 1) * QK_HEAD].T
    values = v_ref[b * BLOCK : (b + 1) * BLOCK, h * V_HEAD : (h + 1) * V_HEAD]
    return matmul((keys.astype(F32) * weight[r : r + 1]).astype(BF16), values)


def summary_kernel(
    place, k_hbm, v_hbm, weight_hbm, gate_hbm, forget_hbm, state_ref, stats_ref, piece0_ref, piece1_ref,
    gate_ref, forget_ref, k_ref, v_ref, sems
):
    size = piece0_ref.shape[0]
    quarter = lambda n: weight_hbm.at[pl.ds(pl.multiple_of((2 * place[1] + n) * size, size), size)]
    copies = fetch(
        [
            (gate_hbm, gate_ref), (forget_hbm, forget_ref), (k_hbm, k_ref), (v_hbm, v_ref),
            (quarter(0), piece0_ref), (quarter(1), piece1_ref),
        ],
        sems,
    )
    copies[0].wait()
    copies[1].wait()
    heads, tokens = gate_ref.shape
    count = tokens // BLOCK
    _, _, total, weight, top = decays(gate_ref[...], forget_ref[...])
    copies[2].wait()
    copies[3].wait()
    stats = []
    for h in range(heads):
        for b in range(count):
            r = h * count + b
            block_state = state_of(k_ref, v_ref, weight, h, b, r)
            if b == 0:
                state, length, stab = block_state, total[r : r + 1], top[r : r + 1]
            else:
                new = jnp.maximum(stab + total[r : r + 1], top[r : r + 1])
                keep = jnp.exp(stab + total[r : r + 1] - new)
                state = state * keep + block_state * jnp.exp(top[r : r + 1] - new)
                length, stab = length + total[r : r + 1], new
        state_ref[h] = state
        stats += [(length, stab)]
    row = [jnp.broadcast_to(s[n], (1, BLOCK)) for n in range(2) for s in stats]
    stats_ref[...] = jnp.concatenate(row + [jnp.zeros((8 - len(row), BLOCK), F32)], axis=0)
    copies[4].wait()
    copies[5].wait()


def local_kernel(
    place, q_hbm, k_hbm, v_hbm, gate_hbm, forget_hbm, local_ref, block_ref, column_ref, row_ref, q_ref, k_ref,
    v_ref, gate_ref, forget_ref, sems
):
    copies = fetch(
        [(gate_hbm, gate_ref), (forget_hbm, forget_ref), (k_hbm, k_ref), (v_hbm, v_ref), (q_hbm, q_ref)], sems
    )
    for copy in copies:
        copy.wait()
    heads, tokens = gate_ref.shape
    count = tokens // BLOCK
    rows = heads * count
    cumulative, gate, total, weight, top = decays(gate_ref[...], forget_ref[...])
    wide = (rows, BLOCK)
    row_ref[...] = jnp.concatenate([jnp.broadcast_to(total, wide), jnp.broadcast_to(top, wide)], axis=0)
    shifted = gate - cumulative
    columns = jnp.concatenate([cumulative] * (BLOCK // rows), axis=0).T
    causal = iota((BLOCK, BLOCK), 0) >= iota((BLOCK, BLOCK), 1)
    lane = iota((BLOCK, BLOCK), 1)
    for h in range(heads):
        for b in range(count):
            r = h * count + b
            block_ref[r] = state_of(k_ref, v_ref, weight, h, b, r)
            part = slice(b * BLOCK, (b + 1) * BLOCK)
            queries = q_ref[part, h * QK_HEAD : (h + 1) * QK_HEAD]
            keys = k_ref[part, h * QK_HEAD : (h + 1) * QK_HEAD]
            values = v_ref[part, h * V_HEAD : (h + 1) * V_HEAD]
            scores = lax.dot_general(queries, keys, (((1,), (1,)), ((), ())), preferred_element_type=F32)
            gaps = jnp.where(causal, columns[:, r : r + 1] + shifted[r : r + 1], VERY_LOW)
            row_max = jnp.max(gaps, axis=1, keepdims=True)
            weights = jnp.where(causal, scores * QK_HEAD**-0.5 * jnp.exp(gaps - row_max), 0.0)
            local_ref[r] = matmul(weights.astype(BF16), values)
            columns = jnp.where(lane == rows + r, row_max, columns)
    column_ref[...] = columns


def joined(first, second):
    stab = jnp.maximum(first[1] + second[0], second[1])
    return first[0] + second[0], stab, jnp.exp(first[1] + second[0] - stab), jnp.exp(second[1] - stab)


def pair_kernel(place, own_ref, other_ref, own_stats, other_stats, meta_ref, out_ref):
    low_core = place[1] == 0
    rows = []
    factors = []
    for h in range(2):
        own = (own_stats[h : h + 1], own_stats[2 + h : 3 + h])
        other = (other_stats[h : h + 1], other_stats[2 + h : 3 + h])
        first = [jnp.where(low_core, a, b) for a, b in zip(own, other)]
        second = [jnp.where(low_core, b, a) for a, b in zip(own, other)]
        total, stab, keep, add = joined(first, second)
        rows.append((total, stab))
        factors.append((jnp.where(low_core, keep, add), jnp.where(low_core, add, keep)))
    mine = jnp.where(low_core, factors[0][0], factors[1][0])[:, :1]
    theirs = jnp.where(low_core, factors[0][1], factors[1][1])[:, :1]
    state = own_ref[place[1]] * mine + other_ref[place[1]] * theirs
    lane = iota((1, BLOCK), 1)
    stats = jnp.zeros((1, BLOCK), F32)
    for n, value in enumerate([rows[0][0], rows[1][0], rows[0][1], rows[1][1]]):
        stats = jnp.where(lane == n, value, stats)
    meta = meta_ref[...]
    zero = jnp.zeros((1, BLOCK), F32)
    line = [*parts_of(stats), meta[0:1], meta[1:2], *parts_of(meta[2:3]), *parts_of(meta[3:4]), zero]
    block = jnp.concatenate(
        [jnp.concatenate(line[2 * n : 2 * n + 2], axis=1) for n in range(6)] + [jnp.zeros((2, 2 * BLOCK), F32)],
        axis=0,
    )
    chips, size = out_ref.shape[0], out_ref.shape[1] // 3
    for chip in range(chips):
        high, low = in_two(state[chip * size : (chip + 1) * size])
        out_ref[chip] = jnp.concatenate([high, low, block], axis=0).astype(BF16)


def prefix_kernel(place, in_ref, out_ref, table_ref, enter_ref):
    low_core = place[1] == 0
    level = place[0]
    chips, size = in_ref.shape[0], in_ref.shape[1] // 3
    state = jnp.zeros((size, in_ref.shape[2]), F32)
    stab = [jnp.zeros((1, 1), F32)] * 2
    enter = [jnp.zeros((1, 1), F32)] * 2
    for chip in range(chips):
        arrived = in_ref[chip].astype(F32)
        piece, meta = arrived[:size] + arrived[size : 2 * size], arrived[2 * size :]
        line = [meta[n // 2 : n // 2 + 1, (n % 2) * BLOCK : (n % 2 + 1) * BLOCK] for n in range(12)]
        stats = line[0] + line[1] + line[2]
        table_ref[chip] = jnp.concatenate(
            [line[3], line[4], line[5] + line[6] + line[7], line[8] + line[9] + line[10]], axis=0
        )
        out_ref[chip] = jnp.concatenate(in_two(state), axis=0).astype(BF16)
        factors = []
        for h in range(2):
            enter[h] = jnp.where(level == chip, stab[h], enter[h])
            total, top = stats[:, h : h + 1], stats[:, 2 + h : 3 + h]
            new = jnp.maximum(total + stab[h], top)
            factors.append((jnp.exp(total + stab[h] - new), jnp.exp(top - new)))
            stab[h] = new
        keep = jnp.where(low_core, factors[0][0], factors[1][0])
        add = jnp.where(low_core, factors[0][1], factors[1][1])
        state = state * keep + piece * add
    row = [jnp.broadcast_to(e, (1, BLOCK)) for e in enter]
    enter_ref[...] = jnp.concatenate(row + [jnp.zeros((8 - len(row), BLOCK), F32)], axis=0)


def cell_kernel(place, *refs):
    fetched, (own_enter, other_enter), outs = refs[:9], refs[9:11], refs[11:-11]
    held, sems, blocks = refs[-11:-2], refs[-2], refs[-1]
    copies = fetch(list(zip(fetched, held)), sems)
    row_ref, column_ref, other_stats, enter_ref, gain_ref, q_ref, other_state, local_ref, block_ref = held
    for copy in copies[:-2]:
        copy.wait()
    low_core = place[1] == 0
    lane = place[2]
    count = q_ref.shape[0] // BLOCK
    rows = row_ref.shape[0] // 2
    heads = rows // count
    scale = QK_HEAD**-0.5
    columns = column_ref[...]
    for h in range(heads):
        entering = jnp.where(place[1] == h, own_enter[...].astype(F32), other_enter[...].astype(F32))
        size = entering.shape[1] // 2
        entering = (entering[:, :size] + entering[:, size:]).reshape(QK_HEAD, V_HEAD)
        stab = enter_ref[h : h + 1, :1]
        total, top = other_stats[h : h + 1, :1], other_stats[2 + h : 3 + h, :1]
        new = jnp.maximum(stab + total, top)
        keep = jnp.where(low_core, 1.0, jnp.exp(stab + total - new))
        add = jnp.where(low_core, 0.0, jnp.exp(top - new))
        stab = jnp.where(low_core, stab, new)
        state = entering * keep + other_state[h] * add
        for b in range(count):
            r = h * count + b
            queries = q_ref[b * BLOCK : (b + 1) * BLOCK, h * QK_HEAD : (h + 1) * QK_HEAD]
            high = state.astype(BF16)
            low = (state - high.astype(F32)).astype(BF16)
            readout = (matmul(queries, high) + matmul(queries, low)) * scale
            if r == 0:
                copies[-2].wait()
                copies[-1].wait()
            row_max = columns[:, rows + r : rows + r + 1]
            inter = columns[:, r : r + 1] + stab
            top_t = jnp.maximum(inter, row_max)
            cell = jnp.exp(row_max - top_t) * local_ref[r] + jnp.exp(inter - top_t) * readout
            cell = cell * lax.rsqrt(jnp.mean(cell * cell, axis=1, keepdims=True) + EPSILON)
            part = slice(h * V_HEAD, (h + 1) * V_HEAD)
            blocks[b, :, part] = (cell * gain_ref[:, part]).astype(BF16)
            if b + 1 < count:
                total, top = row_ref[r : r + 1, :1], row_ref[rows + r : rows + r + 1, :1]
                new = jnp.maximum(total + stab, top)
                state = state * jnp.exp(total + stab - new) + block_ref[r] * jnp.exp(top - new)
                stab = new
    for slot, out in enumerate(outs):
        out[...] = blocks[lax.rem(slot + lane, count)]


def earlier():
    return (iota((BLOCK, BLOCK), 0) < iota((BLOCK, BLOCK), 1)).astype(BF16)


def routes_kernel(lanes, place, table_ref, own_ref, pack_ref, unpack_ref, select_ref, high_ref, low_ref, fit_ref, held, shares):
    level, core, lane = place[0], place[1], place[2]
    sign = 1 - 2 * core
    chips = table_ref.shape[0]
    plane = 2 * lanes
    before = earlier()
    found = [table_ref[lax.rem(level - sign * d + 2 * chips, chips)] for d in ORIGINS]
    first, second, share0, share1 = (
        jnp.concatenate([f[n : n + 1] for f in found], axis=0) for n in range(4)
    )
    first, second = first.astype(jnp.int32), second.astype(jnp.int32)
    most = jnp.zeros((1, 1), F32)
    for p in range(chips):
        named = (first // plane == p) | (second // plane == p)
        most = jnp.maximum(most, jnp.max(jnp.sum(named.astype(F32), axis=1, keepdims=True), axis=0, keepdims=True))
    fit_ref[...] = jnp.broadcast_to((most <= PLANE_ROWS).astype(F32), fit_ref.shape)

    def code(ids):
        local = ids - plane * level
        inside = (local >= 0) & (local < plane)
        across = lax.rem(lax.rem(local + plane * chips, lanes) - lane + lanes, lanes)
        other = jnp.where(local // lanes == core, 0, 1)
        return jnp.where(inside, across * 2 + other, -1)

    code0, code1 = code(first), code(second)
    hits = [(code0 == j) | (code1 == j) for j in range(plane)]
    marks = jnp.concatenate([h.astype(F32) for h in hits], axis=0)
    slot = matmul(marks.astype(BF16), before)
    weight = jnp.concatenate(
        [jnp.where(code0 == j, share0, 0.0) + jnp.where(code1 == j, share1, 0.0) for j in range(plane)], axis=0
    )
    wanted = ((code0 >= 0) | (code1 >= 0)).astype(F32)
    row = matmul(wanted.astype(BF16), before)
    row_no = iota((PLANE_ROWS, BLOCK), 0).astype(F32)
    slot_no = iota((SLOTS, BLOCK), 0).astype(F32)
    for o in range(chips):
        group, place_in = divmod(o, GROUP)
        rows = jnp.where((row[o : o + 1] == row_no) & (wanted[o : o + 1] > 0.5), 1.0, 0.0)
        zero = jnp.zeros((PLANE_ROWS, BLOCK), F32)
        padded = jnp.concatenate([rows if n == place_in else zero for n in range(GROUP)], axis=0)
        placed, value = [], []
        for j in range(plane):
            n = j * chips + o
            there = jnp.where((slot[n : n + 1] == slot_no) & (marks[n : n + 1] > 0.5), 1.0, 0.0)
            placed.append(there)
            value.append(jnp.sum(there * weight[n : n + 1], axis=1, keepdims=True))
        placed = jnp.concatenate(placed, axis=0).astype(BF16)
        pick = lax.dot_general(
            placed, padded.astype(BF16), (((1,), (1,)), ((), ())), preferred_element_type=F32
        )
        for j in range(plane):
            held[group, (j * GROUP + place_in) * SLOTS : (j * GROUP + place_in + 1) * SLOTS] = pick[
                j * SLOTS : (j + 1) * SLOTS
            ]
            shares[group, (j * GROUP + place_in) * SLOTS : (j * GROUP + place_in + 1) * SLOTS] = jnp.broadcast_to(
                value[j], (SLOTS, BLOCK)
            )
    for group in range(chips // GROUP):
        picked = held[group]
        select_ref[group] = picked.astype(BF16)
        back = (picked * shares[group]).T
        high = back.astype(BF16)
        high_ref[group] = high
        low_ref[group] = (back - high.astype(F32)).astype(BF16)
    own = own_ref[...]
    mine0, mine1 = own[0:1].astype(jnp.int32), own[1:2].astype(jnp.int32)
    targets = [lax.rem(level + sign * d + 2 * chips, chips) for d in ORIGINS]
    leaving = jnp.concatenate(
        [((mine0 // plane == t) | (mine1 // plane == t)).astype(F32) for t in targets], axis=0
    )
    leave = matmul(leaving.astype(BF16), before)
    per = BLOCK // PLANE_ROWS
    for part in range(chips // per):
        packs = []
        for n in range(part * per, (part + 1) * per):
            packs.append(jnp.where((leave[n : n + 1] == row_no) & (leaving[n : n + 1] > 0.5), 1.0, 0.0))
        pack = jnp.concatenate(packs, axis=0)
        pack_ref[part * BLOCK : (part + 1) * BLOCK] = pack.astype(BF16)
        unpack_ref[:, part * BLOCK : (part + 1) * BLOCK] = pack.T.astype(BF16)


def project_kernel(place, pack_ref, mixed1, mixed2, mixed3, *refs):
    low_core = place[1] == 0
    fetched, weights, outs = refs[:3], refs[3:16], refs[16:-7]
    mixed0, resid_ref, gain_ref, held, normed_ref, sems, few_sems = refs[-7:]
    mixed = (mixed0, mixed1, mixed2, mixed3)
    few = fetch(list(zip(fetched, (mixed0, resid_ref, gain_ref))), few_sems)
    width = resid_ref.shape[1]
    chunks = sems.shape[0]
    step = width // chunks
    copies = []
    for n in range(chunks):
        part, pairs, at = pl.ds(n * step, step), [], 0
        for w in weights:
            pairs.append((w.at[:, part], held.at[pl.ds(at, w.shape[0]), part]))
            at += w.shape[0]
        copies.append(fetch(pairs, sems.at[n]))
    half = mixed0.shape[1] // 2
    for copy in few:
        copy.wait()
    columns = [mixed0[...]]
    for m in (mixed[1], mixed[3], mixed[2]):
        low, high = m[:, :half], m[:, half:]
        columns += [jnp.where(low_core, low, high), jnp.where(low_core, high, low)]
    columns = jnp.concatenate(columns, axis=1)
    mid_ref, packed = outs[0], outs[1:]
    square = jnp.zeros((resid_ref.shape[0], 1), F32)
    for n in range(chunks):
        part = slice(n * step, (n + 1) * step)
        for copy in copies[n]:
            copy.wait()
        mid = (resid_ref[:, part].astype(F32) + matmul(columns, held[:, part])).astype(BF16)
        mid_ref[:, part] = mid
        mid = mid.astype(F32)
        square = square + jnp.sum(mid * mid, axis=1, keepdims=True)
    factor = lax.rsqrt(square / width + EPSILON)
    for n in range(chunks):
        part = slice(n * step, (n + 1) * step)
        normed_ref[:, part] = (mid_ref[:, part].astype(F32) * factor * gain_ref[:, part]).astype(BF16)
    in_chunks(packed, width, lambda part: matmul(pack_ref[...], normed_ref[:, part]))


def in_chunks(outs, width, product):
    step = width // 4
    size = outs[0].shape[0]
    for n in range(4):
        part = slice(n * step, (n + 1) * step)
        rows = product(part).astype(BF16)
        for number, out in enumerate(outs):
            out[:, part] = rows[number * size : (number + 1) * size]


def select_kernel(place, select_ref, *refs):
    ins, outs = refs[:GROUP], refs[GROUP:]
    rows = lambda part: jnp.concatenate([r[:, part] for r in ins], axis=0)
    in_chunks(outs, ins[0].shape[1], lambda part: matmul(select_ref[...], rows(part)))


def back_kernel(lanes, place, high_ref, low_ref, *refs):
    ins, outs = refs[:lanes], refs[lanes:]

    def product(part):
        rows = jnp.concatenate([r[:, part] for r in ins], axis=0)
        return matmul(high_ref[...], rows) + matmul(low_ref[...], rows)

    in_chunks(outs, ins[0].shape[1], product)


def add_kernel(at, place, unpack_ref, mid_ref, *refs):
    ins, out = refs[:-1], refs[-1]
    step = out.shape[1] // 4
    for n in range(4):
        part = slice(n * step, (n + 1) * step)
        rows = jnp.concatenate([r[:, part] for r in ins], axis=0)
        picks = unpack_ref[:, at : at + rows.shape[0]]
        out[:, part] = (mid_ref[:, part].astype(F32) + matmul(picks, rows)).astype(out.dtype)


def ffn_kernel(lanes, place, *refs):
    ins, weights, outs = refs[:lanes], refs[lanes : lanes + 6], refs[lanes + 6 : 2 * lanes + 6]
    rows, hidden = refs[2 * lanes + 6 :]
    half = ins[0].shape[0] // 2
    width, inner = weights[0].shape
    for which in range(2):
        gates, uppers, downs = weights[3 * which : 3 * which + 3]
        rows[...] = jnp.concatenate([r[which * half : (which + 1) * half] for r in ins], axis=0)

        @pl.loop(0, inner, step=256)
        def _(at):
            part = pl.ds(pl.multiple_of(at, 256), 256)
            gate = matmul(rows[...], gates[:, part])
            upper = matmul(rows[...], uppers[:, part])
            hidden[:, part] = (gate * jax.nn.sigmoid(gate) * upper).astype(BF16)

        @pl.loop(0, width, step=512)
        def _(at):
            part = pl.ds(pl.multiple_of(at, 512), 512)
            result = matmul(hidden[...], downs[:, part]).astype(BF16)
            for number, out in enumerate(outs):
                out[which * half : (which + 1) * half, part] = result[number * half : (number + 1) * half]


def across(pieces, way):
    lanes = len(pieces)
    got = [pieces[0]] * lanes
    for step in sorted(range(1, lanes), key=lambda n: -min(n, lanes - n)):
        got[step] = lax.ppermute(pieces[step], "tp", lane_shift(way * step))
    return got


def gathered_weight(out_weight, quarters):
    below = [lax.ppermute(q, "tp", lane_shift(1)) for q in quarters]
    above = [lax.ppermute(q, "tp", lane_shift(-1)) for q in quarters]
    far = [lax.ppermute(below[0], "tp", lane_shift(1)), lax.ppermute(above[1], "tp", lane_shift(-1))]
    swap = lambda pair: [lax.ppermute(w, "sp", core_pairs()) for w in pair]
    return [out_weight, *below, *swap(below), *above, *swap(above), *far, *swap(far)]


def expert_ffn(arrived, gate_weight, up_weight, down_weight):
    width = arrived.shape[-1]
    flat = arrived.reshape(-1, width)
    gate = matmul(flat, gate_weight[0])
    upper = matmul(flat, up_weight[0])
    hidden = (jax.nn.silu(gate) * upper).astype(BF16)
    return matmul(hidden, down_weight[0]).astype(BF16).reshape(arrived.shape)


def slots_path(normed, mid, expert_ids, share, gate_weight, up_weight, down_weight):
    shard, width = normed.shape
    expert_group = lax.axis_size("sp") * lax.axis_size("tp")
    assigns = expert_ids.reshape(-1)
    assign_count = assigns.shape[0]
    slots_each = CAP_FACTOR * assign_count // expert_group
    one_hot = (assigns[:, None] == jnp.arange(expert_group, dtype=jnp.int32)[None, :]).astype(BF16)
    earlier_mask = jnp.tril(jnp.ones((assign_count, assign_count), BF16), -1)
    counts_before = matmul(earlier_mask, one_hot)
    slot = jnp.sum(counts_before * one_hot.astype(F32), axis=1).astype(jnp.int32)
    target = assigns * slots_each + slot
    filler = (
        jnp.full((expert_group * slots_each,), -1, jnp.int32)
        .at[target]
        .set(jnp.arange(assign_count, dtype=jnp.int32))
    )
    rows_from = jnp.maximum(filler, 0) // TOPK
    outgoing = jnp.where((filler >= 0)[:, None], normed[rows_from], jnp.zeros((), BF16))
    outgoing = outgoing.reshape(expert_group, slots_each, width)
    served = expert_ffn(
        lax.all_to_all(outgoing, ("sp", "tp"), split_axis=0, concat_axis=0, tiled=True),
        gate_weight,
        up_weight,
        down_weight,
    )
    returned = lax.all_to_all(served, ("sp", "tp"), split_axis=0, concat_axis=0, tiled=True)
    picked = returned.reshape(expert_group * slots_each, width)[target]
    picked = picked.reshape(shard, TOPK, width).astype(F32)
    total = jnp.sum(share[:, :, None] * picked, axis=1)
    return (mid.astype(F32) + total).astype(BF16)


def layer(
    queries, keys, values, in_gate, forget_gate, head_gain, out_weight, resid, norm_gain, expert_ids,
    expert_mix, gate_weight, up_weight, down_weight,
):
    tokens = queries.shape[0]
    heads = in_gate.shape[0]
    count = tokens // BLOCK
    lanes = lax.axis_size("tp")
    chips = lax.axis_size("sp") // 2
    shard, width = resid.shape

    gates = [pltpu.VMEM(in_gate.shape, F32), pltpu.VMEM(forget_gate.shape, F32)]
    of_keys = [pltpu.VMEM(keys.shape, BF16), pltpu.VMEM(values.shape, BF16)]
    state, stats, *quarters = call(
        summary_kernel,
        [
            struct((heads, QK_HEAD, V_HEAD), F32),
            struct((8, BLOCK), F32),
            struct((out_weight.shape[0] // 4, width), BF16),
            struct((out_weight.shape[0] // 4, width), BF16),
        ],
        [keys, values, out_weight, in_gate, forget_gate],
        1 << 27,
        hbm=range(5),
        scratch=[*gates, *of_keys, pltpu.SemaphoreType.DMA((6,))],
        limit=60 << 20,
    )
    other_state = lax.ppermute(state, "sp", core_pairs())
    other_stats = lax.ppermute(stats, "sp", core_pairs())
    share = expert_mix / jnp.sum(expert_mix, axis=1, keepdims=True)
    meta = jnp.concatenate([expert_ids.T.astype(F32), share.T], axis=0)
    piece = QK_HEAD // chips
    (sent,) = call(
        pair_kernel, [struct((chips, 3 * piece, V_HEAD), BF16)], [state, other_state, stats, other_stats, meta], 1 << 24
    )
    local, blocks, columns, decay = call(
        local_kernel,
        [
            struct((heads * count, BLOCK, V_HEAD), F32),
            struct((heads * count, QK_HEAD, V_HEAD), F32),
            struct((BLOCK, BLOCK), F32),
            struct((2 * heads * count, BLOCK), F32),
        ],
        [queries, keys, values, in_gate, forget_gate],
        1 << 29,
        after=sent,
        hbm=range(5),
        scratch=[pltpu.VMEM(queries.shape, BF16), *of_keys, *gates, pltpu.SemaphoreType.DMA((5,))],
    )
    prefix, table, enter = call(
        prefix_kernel,
        [struct((chips, 2 * piece, V_HEAD), BF16), struct((chips, 4, BLOCK), F32), struct((8, BLOCK), F32)],
        [over_chips(sent)],
        1 << 24,
        after=decay,
    )
    own_enter = over_chips(prefix)
    other_enter = lax.ppermute(own_enter, "sp", core_pairs())

    plane = 2 * lanes
    slots = plane * GROUP * SLOTS
    groups = chips // GROUP
    pack, unpack, select, high, low, fits = call(
        functools.partial(routes_kernel, lanes),
        [
            struct((chips * PLANE_ROWS, shard), BF16),
            struct((shard, chips * PLANE_ROWS), BF16),
            struct((groups, slots, GROUP * PLANE_ROWS), BF16),
            struct((groups, GROUP * PLANE_ROWS, slots), BF16),
            struct((groups, GROUP * PLANE_ROWS, slots), BF16),
            struct((8, BLOCK), F32),
        ],
        [table, meta],
        1 << 27,
        scratch=[pltpu.VMEM((groups, slots, BLOCK), F32)] * 2,
    )
    fits = fits * lax.ppermute(fits, "sp", core_pairs())
    all_fit = fits
    for step in range(1, lanes):
        all_fit = all_fit * lax.ppermute(fits, "tp", lane_shift(step))

    kept = [
        decay, columns, other_stats, enter, head_gain.reshape(1, heads * V_HEAD), queries, other_state, local,
        blocks,
    ]
    mixed = call(
        cell_kernel,
        [struct((BLOCK, heads * V_HEAD), BF16)] * count,
        [*kept, own_enter, other_enter],
        1 << 29,
        hbm=range(9),
        scratch=[
            *(pltpu.VMEM(a.shape, a.dtype) for a in kept), pltpu.SemaphoreType.DMA((9,)),
            pltpu.VMEM((count, BLOCK, heads * V_HEAD), BF16),
        ],
        limit=60 << 20,
    )
    mixed = across(mixed, 1)
    projection = gathered_weight(out_weight, quarters)
    block = struct((PLANE_ROWS, width), BF16)
    mid, *packed = call(
        project_kernel,
        [struct((shard, width), BF16)] + [block] * chips,
        [pack, *mixed[1:], mixed[0], resid, norm_gain.reshape(1, width), *projection],
        1 << 30,
        scratch=[
            pltpu.VMEM(mixed[0].shape, BF16), pltpu.VMEM(resid.shape, BF16), pltpu.VMEM((1, width), F32),
            pltpu.VMEM((width, width), BF16), pltpu.VMEM((shard, width), BF16), pltpu.SemaphoreType.DMA((4, len(projection))),
            pltpu.SemaphoreType.DMA((3,)),
        ],
        hbm=range(4, 7 + len(projection)),
        limit=40 << 20,
    )

    own = (gate_weight[0], up_weight[0], down_weight[0])
    weights = [*own, *(lax.ppermute(w, "sp", core_pairs()) for w in own)]
    lane_rows = struct((2 * GROUP * SLOTS, width), BF16)
    arrived, chosen, exchanged, served, home, results, returned = ({} for _ in range(7))
    arrived[0] = packed[ORIGINS.index(0)]
    last = None
    for item in PLAN:
        kind, n = item[0], int(item[1:])
        members = ORIGINS[n * GROUP : (n + 1) * GROUP]
        if kind == "o":
            arrived[n] = lax.ppermute(packed[ORIGINS.index(n)], "sp", ring_shift(n))
        elif kind == "S":
            chosen[n] = call(
                select_kernel, [lane_rows] * lanes, [select[n], *(arrived[d] for d in members)], 1 << 28, after=last
            )
            last = chosen[n][0]
        elif kind == "x":
            exchanged[n] = across(chosen[n], 1)
        elif kind == "E":
            served[n] = call(
                functools.partial(ffn_kernel, lanes),
                [lane_rows] * lanes,
                [*exchanged[n], *weights],
                1 << 31,
                after=last,
                scratch=[
                    pltpu.VMEM((lanes * GROUP * SLOTS, width), BF16),
                    pltpu.VMEM((lanes * GROUP * SLOTS, own[0].shape[1]), BF16),
                ],
            )
            last = served[n][0]
        elif kind == "h":
            home[n] = across(served[n], -1)
        elif kind == "B":
            results[n] = call(
                functools.partial(back_kernel, lanes), [block] * GROUP, [high[n], low[n], *home[n]], 1 << 29, after=last
            )
            last = results[n][0]
        else:
            group, at = divmod(ORIGINS.index(n), GROUP)
            returned[n] = lax.ppermute(results[group][at], "sp", ring_shift(-n))
    group, at = divmod(ORIGINS.index(0), GROUP)
    returned[0] = results[group][at]
    total = mid
    for n, groups_in in enumerate(SUMS):
        members = [d for g in groups_in for d in ORIGINS[g * GROUP : (g + 1) * GROUP]]
        (total,) = call(
            functools.partial(add_kernel, groups_in[0] * GROUP * PLANE_ROWS),
            [struct((shard, width), BF16 if n + 1 == len(SUMS) else F32)],
            [unpack, total, *(returned[d] for d in members)],
            1 << 29,
            after=last,
        )
    out = total

    def redo(carry):
        again, _ = carry
        middle, routed, again = lax.optimization_barrier((mid, meta, again))
        square = middle.astype(F32)
        factor = lax.rsqrt(jnp.mean(square * square, axis=1, keepdims=True) + EPSILON)
        rows = (square * factor * norm_gain).astype(BF16)
        ids, parts = routed[:TOPK].T.astype(jnp.int32), routed[TOPK:].T
        return again & False, slots_path(rows, middle, ids, parts, gate_weight, up_weight, down_weight)

    return lax.while_loop(lambda carry: carry[0], redo, (all_fit[0, 0] < 0.5, out))[1]


def solution(mesh):
    in_specs = (
        P(("grp", "sp"), "tp"),
        P(("grp", "sp"), "tp"),
        P(("grp", "sp"), "tp"),
        P("tp", ("grp", "sp")),
        P("tp", ("grp", "sp")),
        P("tp"),
        P("tp", None),
        P(("grp", "sp", "tp"), None),
        P(),
        P(("grp", "sp", "tp"), None),
        P(("grp", "sp", "tp"), None),
        P(("sp", "tp"), None, None),
        P(("sp", "tp"), None, None),
        P(("sp", "tp"), None, None),
    )
    out_specs = P(("grp", "sp", "tp"), None)
    return jax.shard_map(layer, mesh=mesh, in_specs=in_specs, out_specs=out_specs, check_vma=False)
```

```python
import functools

import jax
import jax.numpy as jnp
from jax import lax
from jax.experimental import pallas as pl
from jax.experimental.pallas import tpu as pltpu
from jax.sharding import PartitionSpec as P


QK_HEAD = 128
V_HEAD = 256
BLOCK = 128
TOPK = 2
CAP_FACTOR = 4
EPSILON = 1e-06
VERY_LOW = -1e30

PLANE_ROWS = 32
GROUP = 4
SLOTS = 8
ORIGINS = (7, 9, 8, 0, 5, 11, 6, 10, 3, 13, 4, 12, 1, 15, 2, 14)
PLAN = (
    "o2", "o14", "o8", "o9", "o7", "o1", "o15", "o5", "o11", "o6", "o13", "o10", "o12", "S0", "x0", "S3", "o3",
    "o4", "x3", "E0", "h0", "E3", "h3", "B0", "r8", "S1", "x1", "r9", "S2", "r7", "E1", "h1", "x2", "B3", "r15",
    "r2", "B1", "r10", "r5", "E2", "r14", "r6", "h2", "r11", "B2", "r3", "r13", "r4", "r1", "r12",
)

F32, BF16 = jnp.float32, jnp.bfloat16
VMEM = pltpu.VMEM


SUMS = ((0, 1), (2, 3))


def core_pairs():
    return [(i, i ^ 1) for i in range(lax.axis_size("sp"))]


def ring_shift(step):
    size = lax.axis_size("sp")
    return [(i, (i + (2 * step if i % 2 == 0 else -2 * step)) % size) for i in range(size)]


def lane_shift(step):
    size = lax.axis_size("tp")
    return [(i, (i + step) % size) for i in range(size)]


def over_chips(x):
    size = lax.axis_size("sp")
    groups = [list(range(core, size, 2)) for core in range(2)]
    return lax.all_to_all(x, "sp", 0, 0, axis_index_groups=groups, tiled=True)


def call(kernel, outs, operands, flops, after=None, scratch=(), hbm=(), limit=12 << 20):
    specs = [pl.BlockSpec(memory_space=pl.ANY if n in hbm else VMEM) for n in range(len(operands))]
    operands = list(operands)
    if after is not None:
        operands.append(after)
        specs.append(pl.BlockSpec(memory_space=pl.ANY))
    count = len(operands)

    def body(*refs):
        mine = lax.axis_index("sp")
        place = (lax.div(mine, 2), lax.rem(mine, 2), lax.axis_index("tp"))
        kernel(place, *(refs[: count - 1] if after is not None else refs[:count]), *refs[count:])

    return pl.pallas_call(
        body,
        out_shape=outs,
        in_specs=specs,
        out_specs=[pl.BlockSpec(memory_space=VMEM)] * len(outs),
        scratch_shapes=list(scratch),
        cost_estimate=pl.CostEstimate(flops=flops, bytes_accessed=1 << 21, transcendentals=0),
        compiler_params=pltpu.CompilerParams(vmem_limit_bytes=limit),
    )(*operands)


def struct(shape, kind):
    return jax.ShapeDtypeStruct(shape, kind)


def matmul(a, b):
    return jnp.dot(a, b, preferred_element_type=F32)


def parts_of(x):
    high = x.astype(BF16).astype(F32)
    rest = x - high
    middle = rest.astype(BF16).astype(F32)
    return high, middle, (rest - middle).astype(BF16).astype(F32)


def in_two(x):
    high = x.astype(BF16).astype(F32)
    return high, x - high


def iota(shape, dim):
    return lax.broadcasted_iota(jnp.int32, shape, dim)


def fetch(pairs, sems):
    copies = [pltpu.make_async_copy(source, target, sems.at[n]) for n, (source, target) in enumerate(pairs)]
    for copy in copies:
        copy.start()
    return copies


def decays(gate, forget):
    heads, tokens = gate.shape
    count = tokens // BLOCK
    pieces = [(h, b) for h in range(heads) for b in range(count)]

    def cut(whole):
        return jnp.concatenate([whole[h : h + 1, b * BLOCK : (b + 1) * BLOCK] for h, b in pieces], axis=0)

    forget, gate = cut(forget), cut(gate)
    small = jnp.exp(-jnp.abs(forget))
    one_up = 1.0 + small
    exact = one_up == 1.0
    log_up = jnp.where(exact, small, jnp.log(one_up) * small / jnp.where(exact, 1.0, one_up - 1.0))
    log_forget = jnp.minimum(forget, 0.0) - log_up
    upto = (iota((BLOCK, BLOCK), 0) <= iota((BLOCK, BLOCK), 1)).astype(BF16)
    cumulative = sum(matmul(p.astype(BF16), upto) for p in parts_of(log_forget))
    total = cumulative[:, BLOCK - 1 : BLOCK]
    to_end = total - cumulative + gate
    top = jnp.max(to_end, axis=1, keepdims=True)
    return cumulative, gate, total, jnp.exp(to_end - top), top


def fetch(pairs, sems):
    copies = [pltpu.make_async_copy(source, target, sems.at[n]) for n, (source, target) in enumerate(pairs)]
    for copy in copies:
        copy.start()
    return copies


def state_of(k_ref, v_ref, weight, h, b, r):
    keys = k_ref[b * BLOCK : (b + 1) * BLOCK, h * QK_HEAD : (h + 1) * QK_HEAD].T
    values = v_ref[b * BLOCK : (b + 1) * BLOCK, h * V_HEAD : (h + 1) * V_HEAD]
    return matmul((keys.astype(F32) * weight[r : r + 1]).astype(BF16), values)


def summary_kernel(
    place, k_hbm, v_hbm, weight_hbm, gate_hbm, forget_hbm, state_ref, stats_ref, piece0_ref, piece1_ref,
    gate_ref, forget_ref, k_ref, v_ref, sems
):
    size = piece0_ref.shape[0]
    quarter = lambda n: weight_hbm.at[pl.ds(pl.multiple_of((2 * place[1] + n) * size, size), size)]
    copies = fetch(
        [
            (gate_hbm, gate_ref), (forget_hbm, forget_ref), (k_hbm, k_ref), (v_hbm, v_ref),
            (quarter(0), piece0_ref), (quarter(1), piece1_ref),
        ],
        sems,
    )
    copies[0].wait()
    copies[1].wait()
    heads, tokens = gate_ref.shape
    count = tokens // BLOCK
    _, _, total, weight, top = decays(gate_ref[...], forget_ref[...])
    copies[2].wait()
    copies[3].wait()
    stats = []
    for h in range(heads):
        for b in range(count):
            r = h * count + b
            block_state = state_of(k_ref, v_ref, weight, h, b, r)
            if b == 0:
                state, length, stab = block_state, total[r : r + 1], top[r : r + 1]
            else:
                new = jnp.maximum(stab + total[r : r + 1], top[r : r + 1])
                keep = jnp.exp(stab + total[r : r + 1] - new)
                state = state * keep + block_state * jnp.exp(top[r : r + 1] - new)
                length, stab = length + total[r : r + 1], new
        state_ref[h] = state
        stats += [(length, stab)]
    row = [jnp.broadcast_to(s[n], (1, BLOCK)) for n in range(2) for s in stats]
    stats_ref[...] = jnp.concatenate(row + [jnp.zeros((8 - len(row), BLOCK), F32)], axis=0)
    copies[4].wait()
    copies[5].wait()


def local_kernel(
    place, q_hbm, k_hbm, v_hbm, gate_hbm, forget_hbm, local_ref, block_ref, column_ref, row_ref, q_ref, k_ref,
    v_ref, gate_ref, forget_ref, sems
):
    copies = fetch(
        [(gate_hbm, gate_ref), (forget_hbm, forget_ref), (k_hbm, k_ref), (v_hbm, v_ref), (q_hbm, q_ref)], sems
    )
    for copy in copies:
        copy.wait()
    heads, tokens = gate_ref.shape
    count = tokens // BLOCK
    rows = heads * count
    cumulative, gate, total, weight, top = decays(gate_ref[...], forget_ref[...])
    wide = (rows, BLOCK)
    row_ref[...] = jnp.concatenate([jnp.broadcast_to(total, wide), jnp.broadcast_to(top, wide)], axis=0)
    shifted = gate - cumulative
    columns = jnp.concatenate([cumulative] * (BLOCK // rows), axis=0).T
    causal = iota((BLOCK, BLOCK), 0) >= iota((BLOCK, BLOCK), 1)
    lane = iota((BLOCK, BLOCK), 1)
    for h in range(heads):
        for b in range(count):
            r = h * count + b
            block_ref[r] = state_of(k_ref, v_ref, weight, h, b, r)
            part = slice(b * BLOCK, (b + 1) * BLOCK)
            queries = q_ref[part, h * QK_HEAD : (h + 1) * QK_HEAD]
            keys = k_ref[part, h * QK_HEAD : (h + 1) * QK_HEAD]
            values = v_ref[part, h * V_HEAD : (h + 1) * V_HEAD]
            scores = lax.dot_general(queries, keys, (((1,), (1,)), ((), ())), preferred_element_type=F32)
            gaps = jnp.where(causal, columns[:, r : r + 1] + shifted[r : r + 1], VERY_LOW)
            row_max = jnp.max(gaps, axis=1, keepdims=True)
            weights = jnp.where(causal, scores * QK_HEAD**-0.5 * jnp.exp(gaps - row_max), 0.0)
            local_ref[r] = matmul(weights.astype(BF16), values)
            columns = jnp.where(lane == rows + r, row_max, columns)
    column_ref[...] = columns


def joined(first, second):
    stab = jnp.maximum(first[1] + second[0], second[1])
    return first[0] + second[0], stab, jnp.exp(first[1] + second[0] - stab), jnp.exp(second[1] - stab)


def pair_kernel(place, own_ref, other_ref, own_stats, other_stats, meta_ref, out_ref):
    low_core = place[1] == 0
    rows = []
    factors = []
    for h in range(2):
        own = (own_stats[h : h + 1], own_stats[2 + h : 3 + h])
        other = (other_stats[h : h + 1], other_stats[2 + h : 3 + h])
        first = [jnp.where(low_core, a, b) for a, b in zip(own, other)]
        second = [jnp.where(low_core, b, a) for a, b in zip(own, other)]
        total, stab, keep, add = joined(first, second)
        rows.append((total, stab))
        factors.append((jnp.where(low_core, keep, add), jnp.where(low_core, add, keep)))
    mine = jnp.where(low_core, factors[0][0], factors[1][0])[:, :1]
    theirs = jnp.where(low_core, factors[0][1], factors[1][1])[:, :1]
    state = own_ref[place[1]] * mine + other_ref[place[1]] * theirs
    lane = iota((1, BLOCK), 1)
    stats = jnp.zeros((1, BLOCK), F32)
    for n, value in enumerate([rows[0][0], rows[1][0], rows[0][1], rows[1][1]]):
        stats = jnp.where(lane == n, value, stats)
    meta = meta_ref[...]
    zero = jnp.zeros((1, BLOCK), F32)
    line = [*parts_of(stats), meta[0:1], meta[1:2], *parts_of(meta[2:3]), *parts_of(meta[3:4]), zero]
    block = jnp.concatenate(
        [jnp.concatenate(line[2 * n : 2 * n + 2], axis=1) for n in range(6)] + [jnp.zeros((2, 2 * BLOCK), F32)],
        axis=0,
    )
    chips, size = out_ref.shape[0], out_ref.shape[1] // 3
    for chip in range(chips):
        high, low = in_two(state[chip * size : (chip + 1) * size])
        out_ref[chip] = jnp.concatenate([high, low, block], axis=0).astype(BF16)


def prefix_kernel(place, in_ref, out_ref, table_ref, enter_ref):
    low_core = place[1] == 0
    level = place[0]
    chips, size = in_ref.shape[0], in_ref.shape[1] // 3
    state = jnp.zeros((size, in_ref.shape[2]), F32)
    stab = [jnp.zeros((1, 1), F32)] * 2
    enter = [jnp.zeros((1, 1), F32)] * 2
    for chip in range(chips):
        arrived = in_ref[chip].astype(F32)
        piece, meta = arrived[:size] + arrived[size : 2 * size], arrived[2 * size :]
        line = [meta[n // 2 : n // 2 + 1, (n % 2) * BLOCK : (n % 2 + 1) * BLOCK] for n in range(12)]
        stats = line[0] + line[1] + line[2]
        table_ref[chip] = jnp.concatenate(
            [line[3], line[4], line[5] + line[6] + line[7], line[8] + line[9] + line[10]], axis=0
        )
        out_ref[chip] = jnp.concatenate(in_two(state), axis=0).astype(BF16)
        factors = []
        for h in range(2):
            enter[h] = jnp.where(level == chip, stab[h], enter[h])
            total, top = stats[:, h : h + 1], stats[:, 2 + h : 3 + h]
            new = jnp.maximum(total + stab[h], top)
            factors.append((jnp.exp(total + stab[h] - new), jnp.exp(top - new)))
            stab[h] = new
        keep = jnp.where(low_core, factors[0][0], factors[1][0])
        add = jnp.where(low_core, factors[0][1], factors[1][1])
        state = state * keep + piece * add
    row = [jnp.broadcast_to(e, (1, BLOCK)) for e in enter]
    enter_ref[...] = jnp.concatenate(row + [jnp.zeros((8 - len(row), BLOCK), F32)], axis=0)


def cell_kernel(place, *refs):
    fetched, (own_enter, other_enter), outs = refs[:9], refs[9:11], refs[11:-11]
    held, sems, blocks = refs[-11:-2], refs[-2], refs[-1]
    copies = fetch(list(zip(fetched, held)), sems)
    row_ref, column_ref, other_stats, enter_ref, gain_ref, q_ref, other_state, local_ref, block_ref = held
    for copy in copies[:-2]:
        copy.wait()
    low_core = place[1] == 0
    lane = place[2]
    count = q_ref.shape[0] // BLOCK
    rows = row_ref.shape[0] // 2
    heads = rows // count
    scale = QK_HEAD**-0.5
    columns = column_ref[...]
    for h in range(heads):
        entering = jnp.where(place[1] == h, own_enter[...].astype(F32), other_enter[...].astype(F32))
        size = entering.shape[1] // 2
        entering = (entering[:, :size] + entering[:, size:]).reshape(QK_HEAD, V_HEAD)
        stab = enter_ref[h : h + 1, :1]
        total, top = other_stats[h : h + 1, :1], other_stats[2 + h : 3 + h, :1]
        new = jnp.maximum(stab + total, top)
        keep = jnp.where(low_core, 1.0, jnp.exp(stab + total - new))
        add = jnp.where(low_core, 0.0, jnp.exp(top - new))
        stab = jnp.where(low_core, stab, new)
        state = entering * keep + other_state[h] * add
        for b in range(count):
            r = h * count + b
            queries = q_ref[b * BLOCK : (b + 1) * BLOCK, h * QK_HEAD : (h + 1) * QK_HEAD]
            high = state.astype(BF16)
            low = (state - high.astype(F32)).astype(BF16)
            readout = (matmul(queries, high) + matmul(queries, low)) * scale
            if r == 0:
                copies[-2].wait()
                copies[-1].wait()
            row_max = columns[:, rows + r : rows + r + 1]
            inter = columns[:, r : r + 1] + stab
            top_t = jnp.maximum(inter, row_max)
            cell = jnp.exp(row_max - top_t) * local_ref[r] + jnp.exp(inter - top_t) * readout
            cell = cell * lax.rsqrt(jnp.mean(cell * cell, axis=1, keepdims=True) + EPSILON)
            part = slice(h * V_HEAD, (h + 1) * V_HEAD)
            blocks[b, :, part] = (cell * gain_ref[:, part]).astype(BF16)
            if b + 1 < count:
                total, top = row_ref[r : r + 1, :1], row_ref[rows + r : rows + r + 1, :1]
                new = jnp.maximum(total + stab, top)
                state = state * jnp.exp(total + stab - new) + block_ref[r] * jnp.exp(top - new)
                stab = new
    for slot, out in enumerate(outs):
        out[...] = blocks[lax.rem(slot + lane, count)]


def earlier():
    return (iota((BLOCK, BLOCK), 0) < iota((BLOCK, BLOCK), 1)).astype(BF16)


def routes_kernel(lanes, place, table_ref, own_ref, pack_ref, unpack_ref, select_ref, high_ref, low_ref, fit_ref, held, shares):
    level, core, lane = place[0], place[1], place[2]
    sign = 1 - 2 * core
    chips = table_ref.shape[0]
    plane = 2 * lanes
    before = earlier()
    found = [table_ref[lax.rem(level - sign * d + 2 * chips, chips)] for d in ORIGINS]
    first, second, share0, share1 = (
        jnp.concatenate([f[n : n + 1] for f in found], axis=0) for n in range(4)
    )
    first, second = first.astype(jnp.int32), second.astype(jnp.int32)
    most = jnp.zeros((1, 1), F32)
    for p in range(chips):
        named = (first // plane == p) | (second // plane == p)
        most = jnp.maximum(most, jnp.max(jnp.sum(named.astype(F32), axis=1, keepdims=True), axis=0, keepdims=True))
    fit_ref[...] = jnp.broadcast_to((most <= PLANE_ROWS).astype(F32), fit_ref.shape)

    def code(ids):
        local = ids - plane * level
        inside = (local >= 0) & (local < plane)
        across = lax.rem(lax.rem(local + plane * chips, lanes) - lane + lanes, lanes)
        other = jnp.where(local // lanes == core, 0, 1)
        return jnp.where(inside, across * 2 + other, -1)

    code0, code1 = code(first), code(second)
    hits = [(code0 == j) | (code1 == j) for j in range(plane)]
    marks = jnp.concatenate([h.astype(F32) for h in hits], axis=0)
    slot = matmul(marks.astype(BF16), before)
    weight = jnp.concatenate(
        [jnp.where(code0 == j, share0, 0.0) + jnp.where(code1 == j, share1, 0.0) for j in range(plane)], axis=0
    )
    wanted = ((code0 >= 0) | (code1 >= 0)).astype(F32)
    row = matmul(wanted.astype(BF16), before)
    row_no = iota((PLANE_ROWS, BLOCK), 0).astype(F32)
    slot_no = iota((SLOTS, BLOCK), 0).astype(F32)
    for o in range(chips):
        group, place_in = divmod(o, GROUP)
        rows = jnp.where((row[o : o + 1] == row_no) & (wanted[o : o + 1] > 0.5), 1.0, 0.0)
        zero = jnp.zeros((PLANE_ROWS, BLOCK), F32)
        padded = jnp.concatenate([rows if n == place_in else zero for n in range(GROUP)], axis=0)
        placed, value = [], []
        for j in range(plane):
            n = j * chips + o
            there = jnp.where((slot[n : n + 1] == slot_no) & (marks[n : n + 1] > 0.5), 1.0, 0.0)
            placed.append(there)
            value.append(jnp.sum(there * weight[n : n + 1], axis=1, keepdims=True))
        placed = jnp.concatenate(placed, axis=0).astype(BF16)
        pick = lax.dot_general(
            placed, padded.astype(BF16), (((1,), (1,)), ((), ())), preferred_element_type=F32
        )
        for j in range(plane):
            held[group, (j * GROUP + place_in) * SLOTS : (j * GROUP + place_in + 1) * SLOTS] = pick[
                j * SLOTS : (j + 1) * SLOTS
            ]
            shares[group, (j * GROUP + place_in) * SLOTS : (j * GROUP + place_in + 1) * SLOTS] = jnp.broadcast_to(
                value[j], (SLOTS, BLOCK)
            )
    for group in range(chips // GROUP):
        picked = held[group]
        select_ref[group] = picked.astype(BF16)
        back = (picked * shares[group]).T
        high = back.astype(BF16)
        high_ref[group] = high
        low_ref[group] = (back - high.astype(F32)).astype(BF16)
    own = own_ref[...]
    mine0, mine1 = own[0:1].astype(jnp.int32), own[1:2].astype(jnp.int32)
    targets = [lax.rem(level + sign * d + 2 * chips, chips) for d in ORIGINS]
    leaving = jnp.concatenate(
        [((mine0 // plane == t) | (mine1 // plane == t)).astype(F32) for t in targets], axis=0
    )
    leave = matmul(leaving.astype(BF16), before)
    per = BLOCK // PLANE_ROWS
    for part in range(chips // per):
        packs = []
        for n in range(part * per, (part + 1) * per):
            packs.append(jnp.where((leave[n : n + 1] == row_no) & (leaving[n : n + 1] > 0.5), 1.0, 0.0))
        pack = jnp.concatenate(packs, axis=0)
        pack_ref[part * BLOCK : (part + 1) * BLOCK] = pack.astype(BF16)
        unpack_ref[:, part * BLOCK : (part + 1) * BLOCK] = pack.T.astype(BF16)


def project_kernel(place, pack_ref, mixed1, mixed2, mixed3, *refs):
    low_core = place[1] == 0
    fetched, weights, outs = refs[:3], refs[3:16], refs[16:-7]
    mixed0, resid_ref, gain_ref, held, normed_ref, sems, few_sems = refs[-7:]
    mixed = (mixed0, mixed1, mixed2, mixed3)
    few = fetch(list(zip(fetched, (mixed0, resid_ref, gain_ref))), few_sems)
    width = resid_ref.shape[1]
    chunks = sems.shape[0]
    step = width // chunks
    copies = []
    for n in range(chunks):
        part, pairs, at = pl.ds(n * step, step), [], 0
        for w in weights:
            pairs.append((w.at[:, part], held.at[pl.ds(at, w.shape[0]), part]))
            at += w.shape[0]
        copies.append(fetch(pairs, sems.at[n]))
    half = mixed0.shape[1] // 2
    for copy in few:
        copy.wait()
    columns = [mixed0[...]]
    for m in (mixed[1], mixed[3], mixed[2]):
        low, high = m[:, :half], m[:, half:]
        columns += [jnp.where(low_core, low, high), jnp.where(low_core, high, low)]
    columns = jnp.concatenate(columns, axis=1)
    mid_ref, packed = outs[0], outs[1:]
    square = jnp.zeros((resid_ref.shape[0], 1), F32)
    for n in range(chunks):
        part = slice(n * step, (n + 1) * step)
        for copy in copies[n]:
            copy.wait()
        mid = (resid_ref[:, part].astype(F32) + matmul(columns, held[:, part])).astype(BF16)
        mid_ref[:, part] = mid
        mid = mid.astype(F32)
        square = square + jnp.sum(mid * mid, axis=1, keepdims=True)
    factor = lax.rsqrt(square / width + EPSILON)
    for n in range(chunks):
        part = slice(n * step, (n + 1) * step)
        normed_ref[:, part] = (mid_ref[:, part].astype(F32) * factor * gain_ref[:, part]).astype(BF16)
    in_chunks(packed, width, lambda part: matmul(pack_ref[...], normed_ref[:, part]))


def in_chunks(outs, width, product):
    step = width // 4
    size = outs[0].shape[0]
    for n in range(4):
        part = slice(n * step, (n + 1) * step)
        rows = product(part).astype(BF16)
        for number, out in enumerate(outs):
            out[:, part] = rows[number * size : (number + 1) * size]


def select_kernel(group, place, select_ref, *refs):
    ins, outs = refs[:GROUP], refs[GROUP:]
    rows = lambda part: jnp.concatenate([r[:, part] for r in ins], axis=0)
    in_chunks(outs, ins[0].shape[1], lambda part: matmul(select_ref[group], rows(part)))


def back_kernel(lanes, group, place, high_ref, low_ref, *refs):
    ins, outs = refs[:lanes], refs[lanes:]

    def product(part):
        rows = jnp.concatenate([r[:, part] for r in ins], axis=0)
        return matmul(high_ref[group], rows) + matmul(low_ref[group], rows)

    in_chunks(outs, ins[0].shape[1], product)


def add_kernel(at, place, unpack_ref, mid_ref, *refs):
    ins, out = refs[:-1], refs[-1]
    step = out.shape[1] // 4
    for n in range(4):
        part = slice(n * step, (n + 1) * step)
        rows = jnp.concatenate([r[:, part] for r in ins], axis=0)
        picks = unpack_ref[:, at : at + rows.shape[0]]
        out[:, part] = (mid_ref[:, part].astype(F32) + matmul(picks, rows)).astype(out.dtype)


def ffn_kernel(lanes, place, *refs):
    ins, weights, outs = refs[:lanes], refs[lanes : lanes + 6], refs[lanes + 6 : 2 * lanes + 6]
    rows, hidden = refs[2 * lanes + 6 :]
    half = ins[0].shape[0] // 2
    width, inner = weights[0].shape
    for which in range(2):
        gates, uppers, downs = weights[3 * which : 3 * which + 3]
        rows[...] = jnp.concatenate([r[which * half : (which + 1) * half] for r in ins], axis=0)

        @pl.loop(0, inner, step=256)
        def _(at):
            part = pl.ds(pl.multiple_of(at, 256), 256)
            gate = matmul(rows[...], gates[:, part])
            upper = matmul(rows[...], uppers[:, part])
            hidden[:, part] = (gate * jax.nn.sigmoid(gate) * upper).astype(BF16)

        @pl.loop(0, width, step=512)
        def _(at):
            part = pl.ds(pl.multiple_of(at, 512), 512)
            result = matmul(hidden[...], downs[:, part]).astype(BF16)
            for number, out in enumerate(outs):
                out[which * half : (which + 1) * half, part] = result[number * half : (number + 1) * half]


def across(pieces, way):
    lanes = len(pieces)
    got = [pieces[0]] * lanes
    for step in sorted(range(1, lanes), key=lambda n: -min(n, lanes - n)):
        got[step] = lax.ppermute(pieces[step], "tp", lane_shift(way * step))
    return got


def gathered_weight(out_weight, quarters):
    below = [lax.ppermute(q, "tp", lane_shift(1)) for q in quarters]
    above = [lax.ppermute(q, "tp", lane_shift(-1)) for q in quarters]
    far = [lax.ppermute(below[0], "tp", lane_shift(1)), lax.ppermute(above[1], "tp", lane_shift(-1))]
    swap = lambda pair: [lax.ppermute(w, "sp", core_pairs()) for w in pair]
    return [out_weight, *below, *swap(below), *above, *swap(above), *far, *swap(far)]


def expert_ffn(arrived, gate_weight, up_weight, down_weight):
    width = arrived.shape[-1]
    flat = arrived.reshape(-1, width)
    gate = matmul(flat, gate_weight[0])
    upper = matmul(flat, up_weight[0])
    hidden = (jax.nn.silu(gate) * upper).astype(BF16)
    return matmul(hidden, down_weight[0]).astype(BF16).reshape(arrived.shape)


def slots_path(normed, mid, expert_ids, share, gate_weight, up_weight, down_weight):
    shard, width = normed.shape
    expert_group = lax.axis_size("sp") * lax.axis_size("tp")
    assigns = expert_ids.reshape(-1)
    assign_count = assigns.shape[0]
    slots_each = CAP_FACTOR * assign_count // expert_group
    one_hot = (assigns[:, None] == jnp.arange(expert_group, dtype=jnp.int32)[None, :]).astype(BF16)
    earlier_mask = jnp.tril(jnp.ones((assign_count, assign_count), BF16), -1)
    counts_before = matmul(earlier_mask, one_hot)
    slot = jnp.sum(counts_before * one_hot.astype(F32), axis=1).astype(jnp.int32)
    target = assigns * slots_each + slot
    filler = (
        jnp.full((expert_group * slots_each,), -1, jnp.int32)
        .at[target]
        .set(jnp.arange(assign_count, dtype=jnp.int32))
    )
    rows_from = jnp.maximum(filler, 0) // TOPK
    outgoing = jnp.where((filler >= 0)[:, None], normed[rows_from], jnp.zeros((), BF16))
    outgoing = outgoing.reshape(expert_group, slots_each, width)
    served = expert_ffn(
        lax.all_to_all(outgoing, ("sp", "tp"), split_axis=0, concat_axis=0, tiled=True),
        gate_weight,
        up_weight,
        down_weight,
    )
    returned = lax.all_to_all(served, ("sp", "tp"), split_axis=0, concat_axis=0, tiled=True)
    picked = returned.reshape(expert_group * slots_each, width)[target]
    picked = picked.reshape(shard, TOPK, width).astype(F32)
    total = jnp.sum(share[:, :, None] * picked, axis=1)
    return (mid.astype(F32) + total).astype(BF16)


def layer(
    queries, keys, values, in_gate, forget_gate, head_gain, out_weight, resid, norm_gain, expert_ids,
    expert_mix, gate_weight, up_weight, down_weight,
):
    tokens = queries.shape[0]
    heads = in_gate.shape[0]
    count = tokens // BLOCK
    lanes = lax.axis_size("tp")
    chips = lax.axis_size("sp") // 2
    shard, width = resid.shape

    gates = [pltpu.VMEM(in_gate.shape, F32), pltpu.VMEM(forget_gate.shape, F32)]
    of_keys = [pltpu.VMEM(keys.shape, BF16), pltpu.VMEM(values.shape, BF16)]
    state, stats, *quarters = call(
        summary_kernel,
        [
            struct((heads, QK_HEAD, V_HEAD), F32),
            struct((8, BLOCK), F32),
            struct((out_weight.shape[0] // 4, width), BF16),
            struct((out_weight.shape[0] // 4, width), BF16),
        ],
        [keys, values, out_weight, in_gate, forget_gate],
        1 << 27,
        hbm=range(5),
        scratch=[*gates, *of_keys, pltpu.SemaphoreType.DMA((6,))],
        limit=60 << 20,
    )
    other_state = lax.ppermute(state, "sp", core_pairs())
    other_stats = lax.ppermute(stats, "sp", core_pairs())
    share = expert_mix / jnp.sum(expert_mix, axis=1, keepdims=True)
    meta = jnp.concatenate([expert_ids.T.astype(F32), share.T], axis=0)
    piece = QK_HEAD // chips
    (sent,) = call(
        pair_kernel, [struct((chips, 3 * piece, V_HEAD), BF16)], [state, other_state, stats, other_stats, meta], 1 << 24
    )
    local, blocks, columns, decay = call(
        local_kernel,
        [
            struct((heads * count, BLOCK, V_HEAD), F32),
            struct((heads * count, QK_HEAD, V_HEAD), F32),
            struct((BLOCK, BLOCK), F32),
            struct((2 * heads * count, BLOCK), F32),
        ],
        [queries, keys, values, in_gate, forget_gate],
        1 << 29,
        after=sent,
        hbm=range(5),
        scratch=[pltpu.VMEM(queries.shape, BF16), *of_keys, *gates, pltpu.SemaphoreType.DMA((5,))],
    )
    prefix, table, enter = call(
        prefix_kernel,
        [struct((chips, 2 * piece, V_HEAD), BF16), struct((chips, 4, BLOCK), F32), struct((8, BLOCK), F32)],
        [over_chips(sent)],
        1 << 24,
        after=decay,
    )
    own_enter = over_chips(prefix)
    other_enter = lax.ppermute(own_enter, "sp", core_pairs())

    plane = 2 * lanes
    slots = plane * GROUP * SLOTS
    groups = chips // GROUP
    pack, unpack, select, high, low, fits = call(
        functools.partial(routes_kernel, lanes),
        [
            struct((chips * PLANE_ROWS, shard), BF16),
            struct((shard, chips * PLANE_ROWS), BF16),
            struct((groups, slots, GROUP * PLANE_ROWS), BF16),
            struct((groups, GROUP * PLANE_ROWS, slots), BF16),
            struct((groups, GROUP * PLANE_ROWS, slots), BF16),
            struct((8, BLOCK), F32),
        ],
        [table, meta],
        1 << 27,
        scratch=[pltpu.VMEM((groups, slots, BLOCK), F32)] * 2,
    )
    fits = fits * lax.ppermute(fits, "sp", core_pairs())
    all_fit = fits
    for step in range(1, lanes):
        all_fit = all_fit * lax.ppermute(fits, "tp", lane_shift(step))

    kept = [
        decay, columns, other_stats, enter, head_gain.reshape(1, heads * V_HEAD), queries, other_state, local,
        blocks,
    ]
    mixed = call(
        cell_kernel,
        [struct((BLOCK, heads * V_HEAD), BF16)] * count,
        [*kept, own_enter, other_enter],
        1 << 29,
        hbm=range(9),
        scratch=[
            *(pltpu.VMEM(a.shape, a.dtype) for a in kept), pltpu.SemaphoreType.DMA((9,)),
            pltpu.VMEM((count, BLOCK, heads * V_HEAD), BF16),
        ],
        limit=60 << 20,
    )
    mixed = across(mixed, 1)
    projection = gathered_weight(out_weight, quarters)
    block = struct((PLANE_ROWS, width), BF16)
    mid, *packed = call(
        project_kernel,
        [struct((shard, width), BF16)] + [block] * chips,
        [pack, *mixed[1:], mixed[0], resid, norm_gain.reshape(1, width), *projection],
        1 << 30,
        scratch=[
            pltpu.VMEM(mixed[0].shape, BF16), pltpu.VMEM(resid.shape, BF16), pltpu.VMEM((1, width), F32),
            pltpu.VMEM((width, width), BF16), pltpu.VMEM((shard, width), BF16), pltpu.SemaphoreType.DMA((4, len(projection))),
            pltpu.SemaphoreType.DMA((3,)),
        ],
        hbm=range(4, 7 + len(projection)),
        limit=40 << 20,
    )

    own = (gate_weight[0], up_weight[0], down_weight[0])
    weights = [*own, *(lax.ppermute(w, "sp", core_pairs()) for w in own)]
    lane_rows = struct((2 * GROUP * SLOTS, width), BF16)
    arrived, chosen, exchanged, served, home, results, returned = ({} for _ in range(7))
    arrived[0] = packed[ORIGINS.index(0)]
    last = None
    for item in PLAN:
        kind, n = item[0], int(item[1:])
        members = ORIGINS[n * GROUP : (n + 1) * GROUP]
        if kind == "o":
            arrived[n] = lax.ppermute(packed[ORIGINS.index(n)], "sp", ring_shift(n))
        elif kind == "S":
            chosen[n] = call(
                functools.partial(select_kernel, n),
                [lane_rows] * lanes,
                [select, *(arrived[d] for d in members)],
                1 << 28,
                after=last,
            )
            last = chosen[n][0]
        elif kind == "x":
            exchanged[n] = across(chosen[n], 1)
        elif kind == "E":
            served[n] = call(
                functools.partial(ffn_kernel, lanes),
                [lane_rows] * lanes,
                [*exchanged[n], *weights],
                1 << 31,
                after=last,
                scratch=[
                    pltpu.VMEM((lanes * GROUP * SLOTS, width), BF16),
                    pltpu.VMEM((lanes * GROUP * SLOTS, own[0].shape[1]), BF16),
                ],
            )
            last = served[n][0]
        elif kind == "h":
            home[n] = across(served[n], -1)
        elif kind == "B":
            results[n] = call(
                functools.partial(back_kernel, lanes, n), [block] * GROUP, [high, low, *home[n]], 1 << 29, after=last
            )
            last = results[n][0]
        else:
            group, at = divmod(ORIGINS.index(n), GROUP)
            returned[n] = lax.ppermute(results[group][at], "sp", ring_shift(-n))
    group, at = divmod(ORIGINS.index(0), GROUP)
    returned[0] = results[group][at]
    total = mid
    for n, groups_in in enumerate(SUMS):
        members = [d for g in groups_in for d in ORIGINS[g * GROUP : (g + 1) * GROUP]]
        (total,) = call(
            functools.partial(add_kernel, groups_in[0] * GROUP * PLANE_ROWS),
            [struct((shard, width), BF16 if n + 1 == len(SUMS) else F32)],
            [unpack, total, *(returned[d] for d in members)],
            1 << 29,
            after=last,
        )
    out = total

    def redo(carry):
        again, _ = carry
        middle, routed, again = lax.optimization_barrier((mid, meta, again))
        square = middle.astype(F32)
        factor = lax.rsqrt(jnp.mean(square * square, axis=1, keepdims=True) + EPSILON)
        rows = (square * factor * norm_gain).astype(BF16)
        ids, parts = routed[:TOPK].T.astype(jnp.int32), routed[TOPK:].T
        return again & False, slots_path(rows, middle, ids, parts, gate_weight, up_weight, down_weight)

    return lax.while_loop(lambda carry: carry[0], redo, (all_fit[0, 0] < 0.5, out))[1]


def solution(mesh):
    in_specs = (
        P(("grp", "sp"), "tp"),
        P(("grp", "sp"), "tp"),
        P(("grp", "sp"), "tp"),
        P("tp", ("grp", "sp")),
        P("tp", ("grp", "sp")),
        P("tp"),
        P("tp", None),
        P(("grp", "sp", "tp"), None),
        P(),
        P(("grp", "sp", "tp"), None),
        P(("grp", "sp", "tp"), None),
        P(("sp", "tp"), None, None),
        P(("sp", "tp"), None, None),
        P(("sp", "tp"), None, None),
    )
    out_specs = P(("grp", "sp", "tp"), None)
    return jax.shard_map(layer, mesh=mesh, in_specs=in_specs, out_specs=out_specs, check_vma=False)
```
